32 devices in a mesh: sp: 16 (over z, y, x), tp: 2 (over core).
Axes of the slice: x: 2, y: 2, z: 4, core: 2. Of those that a mesh axis runs over, the one named last changes fastest.
Arguments:
- query_proj: bfloat16 [4096, 1024], P('sp', 'tp'), may hold values from -6 to 6
- key_proj: bfloat16 [4096, 512], P('sp', 'tp'), may hold values from -6 to 6
- value_proj: bfloat16 [4096, 512], P('sp', 'tp'), may hold values from -6 to 6
- q_gain: float32 [64], replicated, may hold values from 1.1 to 10, as said below
- k_gain: float32 [64], replicated, may hold values from 1.1 to 10, as said below
- residual: bfloat16 [4096, 2048], P('sp'), may hold values from -6 to 6
- out_weight: bfloat16 [1024, 2048], P('tp'), may hold values from -0.75 to 0.75
- norm_gain: float32 [2048], replicated, may hold values from 0.1 to 1.9
- value_weight: bfloat16 [2048, 5120], P('sp', 'tp'), may hold values from -0.125 to 0.125
- gate_weight: bfloat16 [2048, 5120], P('sp', 'tp'), may hold values from -0.125 to 0.125
- down_weight: bfloat16 [5120, 2048], P('tp', 'sp'), may hold values from -0.078125 to 0.078125
- conv_value: float32 [3, 5120], P(None, 'tp'), may hold values from -3.5 to 3.5
- conv_gate: float32 [3, 5120], P(None, 'tp'), may hold values from -3.5 to 3.5
Outputs:
- layer_out: bfloat16 [4096, 2048], P(('sp', 'tp'))
The draws below stay inside these ranges and needn't reach their ends.
Inputs may be any that keep to these rules, and one draw needn't show every extreme that they name: `q_gain`: per-dimension gains of the query norm. `k_gain`: per-dimension gains of the key norm.
All inputs are finite; a program needn't handle non-finite values.
Results may differ from the reference program's by a relative error of at most 0.015.
The reference program's roundings to bfloat16 on the way count: a program that leaves them out, or rounds other values in their place, can miss the bound.
Values may be sent and summed in bfloat16 or wider, within the bound.
A program may use at most 128 MiB of HBM per device.

```python
import math
import jax
import jax.numpy as jnp
from jax import lax

D = 2048
HEADS = 16
KV_HEADS = 8
HEAD_DIM = 64
FF = 5120
GRID_W = 64
CONV_W = 3
SEQ = 4096
N_TP = 2


def gain_draw(key, salt_value):
    key_here = jax.random.fold_in(key, salt_value)
    return jnp.exp(jax.random.uniform(key_here, (HEAD_DIM,), jnp.float32, jnp.log(1.1), jnp.log(2.0)))


def draw_q_gain(key, part):
    return gain_draw(key, 11)


def draw_k_gain(key, part):
    return gain_draw(key, 23)


def block_scale(key, dims, pieces, least, top_value):
    gain, own = 1.0, jax.random.fold_in(key, 6)
    for axis_at, parts in pieces:
        steps = jnp.exp(jax.random.uniform(jax.random.fold_in(own, axis_at), (parts,), jnp.float32, least / len(pieces), top_value / len(pieces)))
        gain = gain * jnp.repeat(steps, dims[axis_at] // parts).reshape([-1 if axis == axis_at else 1 for axis in range(len(dims))])
    return gain


def centred(rng, extent, width, limit, cuts=(), kind=jnp.bfloat16):
    result = width * jax.random.normal(rng, extent, jnp.float32)
    if cuts:
        result = result * block_scale(rng, extent, cuts, -0.22, 0.18)
    return jnp.clip(result, -limit, limit).astype(kind)


def setup_inputs(seed: int = 0) -> dict:
    splits = jax.random.split(jax.random.key(seed), 14)
    query_proj = centred(splits[0], (SEQ, HEADS * HEAD_DIM), 1.0, 6.0, ((0, 16), (1, 2)))
    key_proj = centred(splits[1], (SEQ, KV_HEADS * HEAD_DIM), 1.0, 6.0, ((0, 16), (1, 2)))
    value_proj = centred(splits[2], (SEQ, KV_HEADS * HEAD_DIM), 1.0, 6.0, ((0, 16), (1, 2)))
    q_gain = draw_q_gain(jax.random.fold_in(splits[13], 71), 0)
    k_gain = draw_k_gain(jax.random.fold_in(splits[13], 71), 0)
    residual = centred(splits[5], (SEQ, D), 1.0, 6.0, ((0, 16),))
    out_weight = centred(splits[6], (HEADS * HEAD_DIM, D), (HEADS * HEAD_DIM // 16) ** -0.5, 0.75, ((0, 2),))
    norm_gain = jnp.clip(1.0 + 0.18 * jax.random.normal(splits[7], (D,), jnp.float32), 0.1, 1.9)
    value_weight = centred(splits[8], (D, FF), D ** -0.5, 0.125, ((0, 16), (1, 2)))
    gate_weight = centred(splits[9], (D, FF), D ** -0.5, 0.125, ((0, 16), (1, 2)))
    down_weight = centred(splits[10], (FF, D), FF ** -0.5, 0.078125, ((0, 2), (1, 16)))
    conv_value = centred(splits[11], (CONV_W, FF), CONV_W ** -0.5, 3.5, ((1, 2),), jnp.float32)
    conv_gate = centred(splits[12], (CONV_W, FF), CONV_W ** -0.5, 3.5, ((1, 2),), jnp.float32)
    return {"query_proj": query_proj, "key_proj": key_proj, "value_proj": value_proj, "q_gain": q_gain, "k_gain": k_gain, "residual": residual, "out_weight": out_weight, "norm_gain": norm_gain, "value_weight": value_weight, "gate_weight": gate_weight, "down_weight": down_weight, "conv_value": conv_value, "conv_gate": conv_gate}


NORM_EPS = 1e-06
ROPE_BASE = 10000.0

def rms_norm(block_in, gain_vec):
    values = block_in.astype(jnp.float32)
    inv_rms = lax.rsqrt(lax.optimization_barrier(jnp.mean(values * values, axis=-1, keepdims=True)) + NORM_EPS)
    return values * inv_rms * gain_vec.astype(jnp.float32)

def rotate_half(values, position):
    full_width = values.shape[-1]
    half_width = full_width // 2
    frequency = ROPE_BASE ** (-jnp.arange(0, full_width, 2, dtype=jnp.float32) / full_width)
    angles = position.astype(jnp.float32)[:, None] * frequency[None, :]
    cosine = jnp.cos(angles)[:, None, :]
    sine_part = jnp.sin(angles)[:, None, :]
    first_half = values[..., :half_width]
    second_half = values[..., half_width:]
    return jnp.concatenate([first_half * cosine - second_half * sine_part, first_half * sine_part + second_half * cosine], axis=-1)

def grid_rotary(values, positions):
    half_width = values.shape[-1] // 2
    grid_row = positions // GRID_W
    column = positions % GRID_W
    return jnp.concatenate([rotate_half(values[..., :half_width], grid_row), rotate_half(values[..., half_width:], column)], axis=-1)

def depthwise(up_rows, tap_weights):
    padded = jnp.pad(up_rows.astype(jnp.float32), ((1, 1), (0, 0)))
    weights = tap_weights.astype(jnp.float32)
    return padded[:-2] * weights[0] + padded[1:-1] * weights[1] + padded[2:] * weights[2]

def reference(query_proj, key_proj, value_proj, q_gain, k_gain, residual, out_weight, norm_gain, value_weight, gate_weight, down_weight, conv_value, conv_gate):
    sequence = query_proj.shape[0]
    positions = jnp.arange(sequence, dtype=jnp.int32)
    group_size = HEADS // KV_HEADS
    queries = grid_rotary(rms_norm(query_proj.reshape(sequence, HEADS, HEAD_DIM), q_gain), positions) * HEAD_DIM ** (-0.5)
    queries = lax.optimization_barrier(queries.astype(jnp.bfloat16)).astype(jnp.float32)
    keys_rot = grid_rotary(rms_norm(key_proj.reshape(sequence, KV_HEADS, HEAD_DIM), k_gain), positions)
    keys_rot = lax.optimization_barrier(keys_rot.astype(jnp.bfloat16)).astype(jnp.float32)
    keys_rep = jnp.repeat(keys_rot, group_size, axis=1)
    values_rep = jnp.repeat(value_proj.reshape(sequence, KV_HEADS, HEAD_DIM).astype(jnp.float32), group_size, axis=1)
    q_span = math.gcd(sequence, 256)

    def attend(q_block):
        scores = jnp.einsum('qhd,shd->hqs', q_block, keys_rep)
        row_max = lax.optimization_barrier(jnp.max(scores, axis=-1, keepdims=True))
        weights = jnp.exp(scores - row_max)
        totals = lax.optimization_barrier(jnp.sum(weights, axis=-1))
        rounded = lax.optimization_barrier(weights.astype(jnp.bfloat16)).astype(jnp.float32)
        summed = jnp.einsum('hqs,shd->qhd', rounded, values_rep)
        return summed / jnp.transpose(totals)[:, :, None]
    results = lax.map(attend, queries.reshape(sequence // q_span, q_span, HEADS, HEAD_DIM))
    attended = results.reshape(sequence, HEADS * HEAD_DIM).astype(jnp.bfloat16)
    head_cols = HEADS * HEAD_DIM // N_TP
    mix_sum = jnp.zeros((sequence, D), jnp.float32)
    for group_index in range(N_TP):
        partial_sum = jnp.dot(attended[:, group_index * head_cols:(group_index + 1) * head_cols], out_weight[group_index * head_cols:(group_index + 1) * head_cols], preferred_element_type=jnp.float32)
        mix_sum = mix_sum + lax.optimization_barrier(partial_sum.astype(jnp.bfloat16)).astype(jnp.float32)
    mix_out = mix_sum.astype(jnp.bfloat16)
    updated = (residual.astype(jnp.float32) + mix_out.astype(jnp.float32)).astype(jnp.bfloat16)
    normed = rms_norm(updated, norm_gain).astype(jnp.bfloat16)
    value_up = jnp.dot(normed, value_weight, preferred_element_type=jnp.float32).astype(jnp.bfloat16)
    gate_up = jnp.dot(normed, gate_weight, preferred_element_type=jnp.float32).astype(jnp.bfloat16)
    conv_val = depthwise(value_up, conv_value)
    conv_gated = depthwise(gate_up, conv_gate)
    hidden = (jax.nn.gelu(conv_gated, approximate=True) * conv_val).astype(jnp.bfloat16)
    ff_cols = FF // N_TP
    branch_sum = jnp.zeros((sequence, D), jnp.float32)
    for group_index in range(N_TP):
        partial_sum = jnp.dot(hidden[:, group_index * ff_cols:(group_index + 1) * ff_cols], down_weight[group_index * ff_cols:(group_index + 1) * ff_cols], preferred_element_type=jnp.float32)
        branch_sum = branch_sum + lax.optimization_barrier(partial_sum.astype(jnp.bfloat16)).astype(jnp.float32)
    branch = branch_sum.astype(jnp.bfloat16)
    return (updated.astype(jnp.float32) + branch.astype(jnp.float32)).astype(jnp.bfloat16)
```

```python
import functools
import math

import jax
import jax.numpy as jnp
from jax import lax
from jax.experimental import pallas as pl
from jax.experimental.pallas import tpu as pltpu
from jax.sharding import PartitionSpec as P


HEAD_DIM = 64
GRID_W = 64


NORM_EPS = 1e-06
ROPE_BASE = 10000.0


def rms_norm(block_in, gain_vec):
    values = block_in.astype(jnp.float32)
    inv_rms = lax.rsqrt(jnp.mean(values * values, axis=-1, keepdims=True) + NORM_EPS)
    return values * inv_rms * gain_vec


def rotate_half(values, position):
    full_width = values.shape[-1]
    half_width = full_width // 2
    frequency = ROPE_BASE ** (-jnp.arange(0, full_width, 2, dtype=jnp.float32) / full_width)
    angles = position.astype(jnp.float32)[:, None] * frequency[None, :]
    cosine = jnp.cos(angles)[:, None, :]
    sine_part = jnp.sin(angles)[:, None, :]
    first_half = values[..., :half_width]
    second_half = values[..., half_width:]
    return jnp.concatenate(
        [
            first_half * cosine - second_half * sine_part,
            first_half * sine_part + second_half * cosine,
        ],
        axis=-1,
    )


def grid_rotary(values, positions):
    half_width = values.shape[-1] // 2
    grid_row = positions // GRID_W
    column = positions % GRID_W
    return jnp.concatenate(
        [
            rotate_half(values[..., :half_width], grid_row),
            rotate_half(values[..., half_width:], column),
        ],
        axis=-1,
    )


def exchange_pieces(block_for, place, count, stride, axis_size):
    received = [block_for(place)]
    for hop in range(1, count):
        block = block_for((place + hop) % count)
        received.append(lax.ppermute(block, "sp", shifted(hop, count, stride, axis_size)))
    return received


def in_place_order(received, place):
    count = len(received)
    doubled = (received[::-1] * 2)[: 2 * count - 1]
    size = received[0].shape[0]
    whole = jnp.concatenate(doubled, axis=0)
    return lax.dynamic_slice_in_dim(whole, (count - 1 - place) * size, count * size, 0)


def shifted(hop, count, stride, axis_size):
    pairs = []
    for source in range(axis_size):
        group, rest = source // stride, source % stride
        pairs.append((source, ((group + hop) % count) * stride + rest))
    return pairs


def spread(block, count, stride):
    pieces = [block]
    for flip in range(1, stride):
        pairs = [
            (group * stride + rest, group * stride + (rest ^ flip))
            for group in range(count)
            for rest in range(stride)
        ]
        pieces.append(lax.ppermute(block, "sp", pairs))
    return pieces


def unflip(pieces, rest):
    bit = 1
    while bit < len(pieces):
        chosen = (rest & bit) != 0
        pieces = [
            jnp.where(chosen, pieces[at ^ bit], pieces[at]) for at in range(len(pieces))
        ]
        bit *= 2
    return pieces


def swap_cores(block):
    return lax.ppermute(block, "tp", [(0, 1), (1, 0)])


def attention_kernel(q_ref, k_ref, vt_ref, out_ref, *, span):
    queries = q_ref[...]
    rows, width = queries.shape
    run_max = jnp.full((1, rows), -1e30, jnp.float32)
    run_sum = jnp.zeros((1, rows), jnp.float32)
    run_acc = jnp.zeros((width, rows), jnp.float32)
    for start in range(0, k_ref.shape[0], span):
        scores = lax.dot_general(
            k_ref[start : start + span, :],
            queries,
            (((1,), (1,)), ((), ())),
            preferred_element_type=jnp.float32,
        )
        new_max = jnp.maximum(run_max, jnp.max(scores, axis=0, keepdims=True))
        probs = jnp.exp(scores - new_max)
        shrink = jnp.exp(run_max - new_max)
        run_sum = run_sum * shrink + jnp.sum(probs, axis=0, keepdims=True)
        run_acc = run_acc * shrink + jnp.dot(
            vt_ref[:, start : start + span],
            probs.astype(jnp.bfloat16),
            preferred_element_type=jnp.float32,
        )
        run_max = new_max
    out_ref[...] = (run_acc / run_sum).T.astype(jnp.bfloat16)


def attend(queries, keys, values_t):
    total, width = queries.shape
    key_count = keys.shape[0]
    block = math.gcd(total, 256)
    return pl.pallas_call(
        functools.partial(attention_kernel, span=math.gcd(key_count, 1024)),
        grid=(total // block,),
        out_shape=jax.ShapeDtypeStruct((total, width), jnp.bfloat16),
        in_specs=[
            pl.BlockSpec((block, width), lambda i: (i, 0)),
            pl.BlockSpec((key_count, width), lambda i: (0, 0)),
            pl.BlockSpec((width, key_count), lambda i: (0, 0)),
        ],
        out_specs=pl.BlockSpec((block, width), lambda i: (i, 0)),
        cost_estimate=pl.CostEstimate(
            flops=16 * total * key_count * width,
            bytes_accessed=4 * (total + key_count) * width,
            transcendentals=total * key_count,
        ),
    )(queries, keys, values_t)


def shards(
    query_proj,
    key_proj,
    value_proj,
    q_gain,
    k_gain,
    residual,
    out_weight,
    norm_gain,
    value_weight,
    gate_weight,
    down_weight,
    conv_value,
    conv_gate,
):
    tokens = query_proj.shape[0]
    heads_here = query_proj.shape[1] // HEAD_DIM
    kv_here = key_proj.shape[1] // HEAD_DIM
    group_size = heads_here // kv_here
    sp_size, tp_size = lax.axis_size("sp"), lax.axis_size("tp")
    count = math.gcd(sp_size, 4)
    stride = sp_size // count
    me, core = lax.axis_index("sp"), lax.axis_index("tp")
    place, rest = me // stride, me % stride
    positions = me * tokens + jnp.arange(tokens, dtype=jnp.int32)

    queries = grid_rotary(
        rms_norm(query_proj.reshape(tokens, heads_here, HEAD_DIM), q_gain), positions
    ) * HEAD_DIM ** (-0.5)
    queries = queries.astype(jnp.bfloat16)
    keys_rot = grid_rotary(
        rms_norm(key_proj.reshape(tokens, kv_here, HEAD_DIM), k_gain), positions
    ).astype(jnp.bfloat16)
    values = value_proj.reshape(tokens, kv_here, HEAD_DIM)

    ff_here = value_weight.shape[1]
    depth_here = value_weight.shape[0]
    hidden_here = ff_here // count

    split_heads = count if kv_here % count == 0 else 1
    kv_each = kv_here // split_heads
    packed = jnp.concatenate(
        [queries.reshape(tokens, kv_here, group_size * HEAD_DIM), keys_rot, values], axis=2
    ).transpose(1, 0, 2)
    packed = packed.reshape(split_heads, kv_each, tokens, (group_size + 2) * HEAD_DIM)
    if split_heads > 1:
        got = exchange_pieces(
            lambda at: lax.dynamic_index_in_dim(packed, at, 0, keepdims=False),
            place,
            count,
            stride,
            sp_size,
        )
        got, weights_in = lax.optimization_barrier((got, (value_weight, gate_weight, down_weight)))
    else:
        got, weights_in = [packed[0]], (value_weight, gate_weight, down_weight)
    value_in, gate_in, down_in = weights_in

    q_width = group_size * HEAD_DIM
    kv_mine = jnp.stack([piece[..., q_width:] for piece in got])
    if split_heads > 1:
        kv_all = jnp.stack(spread(kv_mine, count, stride))
    else:
        kv_all = lax.all_gather(kv_mine, "sp", axis=0)
    kv_all = kv_all.transpose(2 + 0, 0, 1, 3, 4).reshape(kv_each, sp_size * tokens, 2 * HEAD_DIM)

    def up_block(at):
        start = at * hidden_here
        return jnp.concatenate(
            [
                lax.dynamic_slice_in_dim(value_in, start, hidden_here, 1),
                lax.dynamic_slice_in_dim(gate_in, start, hidden_here, 1),
            ],
            axis=1,
        )

    def down_block(at):
        return lax.dynamic_slice_in_dim(down_in, at * hidden_here, hidden_here, 0)

    up_got = exchange_pieces(up_block, place, count, stride, sp_size)
    up_pieces = spread(in_place_order(up_got, place), count, stride)
    columns_here = down_weight.shape[1]
    down_got = exchange_pieces(down_block, place, count, stride, sp_size)
    down_cols = in_place_order(down_got, place).reshape(count, hidden_here, columns_here)
    down_cols = jnp.concatenate([down_cols[at] for at in range(count)], axis=1)
    down_pieces = spread(down_cols, count, stride)

    q_pieces = [piece[..., :q_width] for piece in got]
    per_head = []
    for kv_at in range(kv_each):
        keys_h = kv_all[kv_at, :, :HEAD_DIM]
        values_t = kv_all[kv_at, :, HEAD_DIM:].T
        per_group = []
        for group_at in range(group_size):
            columns = slice(group_at * HEAD_DIM, (group_at + 1) * HEAD_DIM)
            q_here = jnp.concatenate([piece[kv_at, :, columns] for piece in q_pieces], axis=0)
            per_group.append(attend(q_here, keys_h, values_t))
        per_head.append(jnp.concatenate(per_group, axis=1))
    done = jnp.concatenate(per_head, axis=1).reshape(len(got), tokens, -1)
    if split_heads > 1:
        back = [done[0]]
        for hop in range(1, count):
            back.append(lax.ppermute(done[hop], "sp", shifted(-hop, count, stride, sp_size)))
        attended = jnp.roll(jnp.stack(back), place, axis=0).transpose(1, 0, 2)
        attended = attended.reshape(tokens, heads_here * HEAD_DIM)
    else:
        attended = done[0]

    row_share = tokens // tp_size
    residual_mine = lax.dynamic_slice_in_dim(residual, core * row_share, row_share, 0)
    if tp_size == 2:
        weight_other = swap_cores(out_weight)
        halves = attended.reshape(2, row_share, heads_here * HEAD_DIM)
        rows_mine = lax.dynamic_index_in_dim(halves, core, 0, keepdims=False)
        rows_other = swap_cores(lax.dynamic_index_in_dim(halves, 1 - core, 0, keepdims=False))
        mix_mine = jnp.dot(rows_mine, out_weight, preferred_element_type=jnp.float32)
        mix_other = jnp.dot(rows_other, weight_other, preferred_element_type=jnp.float32)
        mix_out = (
            mix_mine.astype(jnp.bfloat16).astype(jnp.float32)
            + mix_other.astype(jnp.bfloat16).astype(jnp.float32)
        ).astype(jnp.bfloat16)
    else:
        mix_out = lax.psum_scatter(
            jnp.dot(attended, out_weight, preferred_element_type=jnp.float32).astype(jnp.bfloat16),
            "tp",
            scatter_dimension=0,
            tiled=True,
        )
    updated = (residual_mine.astype(jnp.float32) + mix_out.astype(jnp.float32)).astype(jnp.bfloat16)
    normed = rms_norm(updated, norm_gain).astype(jnp.bfloat16)
    width = normed.shape[1]
    normed = jnp.stack(
        [
            jnp.concatenate(
                [
                    normed[:, (at * stride + flip) * depth_here :][:, :depth_here]
                    for at in range(count)
                ],
                axis=1,
            )
            for flip in range(stride)
        ]
    )

    ups = []
    for hop in range(count):
        rows = normed
        if hop:
            rows = lax.ppermute(normed, "sp", shifted(hop, count, stride, sp_size))
        if tp_size == 2:
            other = swap_cores(rows)
            rows = jnp.concatenate(
                [jnp.where(core == 0, rows, other), jnp.where(core == 0, other, rows)], axis=1
            )
        else:
            rows = lax.all_gather(rows, "tp", axis=1, tiled=True)
        total = 0.0
        for flip in range(stride):
            part = lax.dynamic_index_in_dim(rows, rest ^ flip, 0, keepdims=False)
            total = total + jnp.dot(part, up_pieces[flip], preferred_element_type=jnp.float32)
        ups.append(total.astype(jnp.bfloat16))
    ups = jnp.stack(ups)

    forward = [
        (group * stride + at, group * stride + (at + 1) % stride)
        for group in range(count)
        for at in range(stride)
    ]
    backward = [(target, source) for source, target in forward]
    before = lax.ppermute(ups[:, -1], "sp", forward)
    after = lax.ppermute(ups[:, 0], "sp", backward)
    hops = jnp.arange(count)
    block_at = (place - hops) % count
    no_before = (rest == 0) & (block_at == 0)
    no_after = (rest == stride - 1) & (block_at == count - 1)
    before = jnp.where(rest == 0, jnp.roll(before, -1, axis=0), before)
    after = jnp.where(rest == stride - 1, jnp.roll(after, 1, axis=0), after)
    before = jnp.where(no_before[:, None], 0, before)
    after = jnp.where(no_after[:, None], 0, after)
    padded = jnp.concatenate([before[:, None], ups, after[:, None]], axis=1).astype(jnp.float32)
    taps = jnp.concatenate(
        [
            lax.dynamic_slice_in_dim(conv_value, place * hidden_here, hidden_here, 1),
            lax.dynamic_slice_in_dim(conv_gate, place * hidden_here, hidden_here, 1),
        ],
        axis=1,
    )
    conv = padded[:, :-2] * taps[0] + padded[:, 1:-1] * taps[1] + padded[:, 2:] * taps[2]
    hidden = (
        jax.nn.gelu(conv[..., hidden_here:], approximate=True) * conv[..., :hidden_here]
    ).astype(jnp.bfloat16)

    down_all = jnp.concatenate(down_pieces, axis=1)
    branch = 0.0
    for hop in list(range(1, count)) + [0]:
        partial = jnp.dot(hidden[hop], down_all, preferred_element_type=jnp.float32)
        if tp_size == 2:
            partial = partial.reshape(2, row_share, width)
            mine = lax.dynamic_index_in_dim(partial, core, 0, keepdims=False)
            theirs = lax.dynamic_index_in_dim(partial, 1 - core, 0, keepdims=False)
            other = swap_cores(theirs.astype(jnp.bfloat16))
            mine = mine + other.astype(jnp.float32)
        else:
            mine = lax.psum_scatter(
                partial.astype(jnp.bfloat16), "tp", scatter_dimension=0, tiled=True
            )
        if hop:
            mine = lax.ppermute(
                mine.astype(jnp.bfloat16), "sp", shifted(-hop, count, stride, sp_size)
            )
        branch = branch + mine.astype(jnp.float32)
    branch = branch.astype(jnp.bfloat16)
    span = count * columns_here
    pieces = unflip([branch[:, at * span : (at + 1) * span] for at in range(stride)], rest)
    branch = jnp.concatenate(
        [
            pieces[at][:, group * columns_here : (group + 1) * columns_here]
            for group in range(count)
            for at in range(stride)
        ],
        axis=1,
    )
    return (updated.astype(jnp.float32) + branch.astype(jnp.float32)).astype(jnp.bfloat16)


def fused_kernel(
    q_in, kv_in, res_in, wo_in, gain, wv_in, wg_in, wd_in, taps_v, taps_g, out,
    qraw, qhead, kvbuf, kbuf, vbuf, top, total, acc, att_send, att_all, wo, res, mix_send, mix_recv,
    own_mix, upd, rows, wup, wdown, ups, hidden, part_keep, part_send, part_recv, red_send,
    red_recv, fin, local_sem, send_sem, recv_sem,
):
    sp, core = lax.axis_index("sp"), lax.axis_index("tp")
    x, y, zl, zh = sp % 2, (sp // 2) % 2, (sp // 4) % 2, sp // 8
    fx, fy, fl, fh = 1 - 2 * x, 1 - 2 * y, 1 - 2 * zl, 1 - 2 * zh
    depth = wv_in.shape[0]
    ffs = wdown.shape[1]
    pairs, half, pair_w = out.shape
    tokens = 2 * half
    other = 1 - core

    def xs(flip):
        return x + fx * flip

    def mate(at):
        return sp + fx * (at % 2) + 4 * fl * (at // 2)

    def place(at):
        return xs(at % 2) + 2 * (zl + fl * (at // 2))

    mine = place(0)
    y_mate, z_mate = sp + 2 * fy, sp + 8 * fh
    diag_mate = sp + 2 * fy + 8 * fh

    def pair_at(rel):
        return (y + fy * (rel % 2)) + 2 * (zl + fl * ((rel // 2) % 2)) + 4 * (zh + fh * (rel // 4))

    ids = {}
    started = []

    def remote(name, src, dst, device):
        at = ids.setdefault(name, len(ids))
        assert at < send_sem.shape[0], len(ids)
        return pltpu.make_async_remote_copy(
            src_ref=src, dst_ref=dst, send_sem=send_sem.at[at], recv_sem=recv_sem.at[at],
            device_id=device, device_id_type=pl.DeviceIdType.MESH,
        )

    def send(name, src, dst, device):
        copy = remote(name, src, dst, device)
        copy.start()
        started.append(copy)

    def arrived(name, dst):
        remote(name, dst, dst, (sp, core)).wait_recv()

    def lanes(start, size):
        return pl.ds(pl.multiple_of(start, 128), size)

    barrier = pltpu.get_barrier_semaphore()
    partners = [(sp, other)] + [(mate(at), core) for at in (1, 2, 3)]
    partners += [(y_mate, core), (z_mate, core), (diag_mate, core)]
    for device in partners:
        pl.semaphore_signal(barrier, inc=1, device_id=device, device_id_type=pl.DeviceIdType.MESH)
    pl.semaphore_wait(barrier, len(partners))

    def piece(kind, rel, x_at):
        start = pl.multiple_of(x_at * depth, depth)
        if kind == "v":
            return wup.at[rel, pl.ds(start, depth), pl.ds(0, ffs)]
        if kind == "g":
            return wup.at[rel, pl.ds(start, depth), pl.ds(ffs, ffs)]
        return wdown.at[rel, :, pl.ds(start, depth)]

    def whole(kind, rel):
        if kind == "v":
            return wup.at[rel, :, pl.ds(0, ffs)]
        if kind == "g":
            return wup.at[rel, :, pl.ds(ffs, ffs)]
        return wdown.at[rel]

    def shard(kind, at):
        if kind == "d":
            return wd_in.at[pl.ds(pl.multiple_of(place(at) * ffs, 128), ffs), :]
        return (wv_in if kind == "v" else wg_in).at[:, lanes(place(at) * ffs, ffs)]

    def exchange(kind, at):
        send(f"w1{kind}{at}", shard(kind, at), piece(kind, 2 * (at // 2), x), (mate(at), core))

    def exchanged(kind, at):
        arrived(f"w1{kind}{at}", piece(kind, 2 * (at // 2), xs(at % 2)))

    def across(kind, at):
        src = piece(kind, 2 * (at // 2), xs(at % 2)) if at else shard(kind, 0)
        dst = piece(kind, 2 * (at // 2) + 4, xs(at % 2))
        send(f"wz{kind}{at}", src, dst, (z_mate, core))

    def crossed(kind, at):
        arrived(f"wz{kind}{at}", piece(kind, 2 * (at // 2) + 4, xs(at % 2)))

    def sideways(kind, rel):
        send(f"wy{kind}{rel}", whole(kind, rel), whole(kind, rel + 1), (y_mate, core))

    def from_side(kind, rel):
        arrived(f"wy{kind}{rel}", whole(kind, rel + 1))

    for at in (2, 3, 1):
        send(f"kv{at}", kv_in.at[place(at)], kvbuf.at[0, mine], (mate(at), core))
    for at in (2, 3, 1):
        send(f"q{at}", q_in.at[place(at)], qraw.at[mine], (mate(at), core))
    across("v", 0)
    locals_ = [
        pltpu.make_async_copy(shard(kind, 0), piece(kind, 0, x), local_sem.at[n])
        for n, kind in enumerate("vgd")
    ]
    locals_.append(pltpu.make_async_copy(wo_in, wo, local_sem.at[3]))
    locals_.append(
        pltpu.make_async_copy(
            res_in.at[pl.ds(pl.multiple_of(core * half, half), half), :], res, local_sem.at[4]
        )
    )
    for copy in locals_:
        copy.start()
    for kind in "vgd":
        exchange(kind, 1)
    qraw[mine] = q_in[mine]
    kvbuf[0, mine] = kv_in[mine]
    top[...] = jnp.full(top.shape, -1e30, jnp.float32)
    total[...] = jnp.zeros(total.shape, jnp.float32)
    acc[...] = jnp.zeros(acc.shape, jnp.float32)
    for at in (1, 2, 3):
        arrived(f"kv{at}", kvbuf.at[0, place(at)])
    send("kvz", kvbuf.at[0], kvbuf.at[2], (z_mate, core))
    send("kvy", kvbuf.at[0], kvbuf.at[1], (y_mate, core))
    for at in (2, 3):
        exchange("v", at)
    for at in (1, 2, 3):
        arrived(f"q{at}", qraw.at[place(at)])
    width = HEAD_DIM
    group = qraw.shape[2] // width
    blocks = qraw.shape[0]

    @pl.loop(0, blocks)
    def _(b):
        for a in range(group):
            qhead[b * group + a] = qraw[b][:, a * width : (a + 1) * width]

    def unpack(t):
        @pl.loop(0, blocks)
        def _(b):
            start = pl.multiple_of(b * tokens, tokens)
            pair = kvbuf[t, b]
            kbuf[t, pl.ds(start, tokens), :] = pair[:, :width]
            vbuf[t, :, pl.ds(start, tokens)] = pair[:, width:].T

    def attend_block(t, h):
        scores = lax.dot_general(
            kbuf[t], qhead[h], (((1,), (1,)), ((), ())), preferred_element_type=jnp.float32
        )
        old = top[h]
        new = jnp.maximum(old, jnp.max(scores, axis=0, keepdims=True))
        probs = jnp.exp(scores - new)
        shrink = jnp.exp(old - new)
        total[h] = total[h] * shrink + jnp.sum(probs, axis=0, keepdims=True)
        acc[h] = acc[h] * shrink + jnp.dot(
            vbuf[t], probs.astype(jnp.bfloat16), preferred_element_type=jnp.float32
        )
        top[h] = new

    def attend_some(t, lo, hi):
        @pl.loop(lo, hi)
        def _(h):
            attend_block(t, h)

    heads = blocks * group
    unpack(0)
    attend_some(0, 0, heads // 2)
    locals_[0].wait()
    locals_[1].wait()
    exchanged("v", 1)
    across("v", 1)
    sideways("v", 0)
    attend_some(0, heads // 2, heads)
    for at in (2, 3):
        exchange("g", at)
    arrived("kvy", kvbuf.at[1])
    unpack(1)
    attend_some(1, 0, heads)
    arrived("kvz", kvbuf.at[2])
    send("kvd", kvbuf.at[2], kvbuf.at[3], (y_mate, core))
    across("g", 0)
    exchanged("g", 1)
    sideways("g", 0)
    unpack(2)
    attend_some(2, 0, heads // 2)
    across("g", 1)
    for at in (2, 3):
        exchange("d", at)
    exchanged("v", 2)
    exchanged("v", 3)
    sideways("v", 2)
    attend_some(2, heads // 2, heads)
    arrived("kvd", kvbuf.at[3])
    unpack(3)

    def finish(block):
        first = block * group
        pieces = [acc[first + a] / total[first + a] for a in range(group)]
        return jnp.concatenate(pieces, axis=0).T.astype(jnp.bfloat16)

    for at in (2, 3, 1, 0):
        block = place(at)
        attend_some(3, block * group, block * group + group)
        if at:
            att_send[at - 1] = finish(block)
            send(f"att{at}", att_send.at[at - 1], att_all.at[mine], (mate(at), core))
        else:
            att_all[mine] = finish(block)
    across("v", 2)
    exchanged("g", 2)
    exchanged("g", 3)
    sideways("g", 2)
    locals_[3].wait()
    locals_[4].wait()
    for at in (1, 2, 3):
        arrived(f"att{at}", att_all.at[place(at)])

    def project(n, rows_at):
        start = pl.multiple_of(rows_at * half, half)
        left = jnp.concatenate([att_all[b, pl.ds(start, half), :] for b in range(blocks)], axis=1)
        return jnp.dot(left, wo[:, lanes(n * pair_w, pair_w)], preferred_element_type=jnp.float32)

    @pl.loop(0, pairs)
    def _(n):
        mix_send[n] = project(n, other).astype(jnp.bfloat16)

    send("mix", mix_send, mix_recv, (sp, other))

    @pl.loop(0, pairs)
    def _(n):
        own_mix[n] = project(n, core).astype(jnp.bfloat16)

    arrived("mix", mix_recv)

    def update(n, squares):
        mixed = own_mix[n].astype(jnp.float32) + mix_recv[n].astype(jnp.float32)
        mixed = mixed.astype(jnp.bfloat16).astype(jnp.float32)
        held = res[:, lanes(n * pair_w, pair_w)].astype(jnp.float32)
        new = (held + mixed).astype(jnp.bfloat16)
        upd[n] = new
        wide = new.astype(jnp.float32)
        return squares + jnp.sum(wide * wide, axis=1, keepdims=True)

    squares = lax.fori_loop(0, pairs, update, jnp.zeros((half, 1), jnp.float32))
    inv = lax.rsqrt(squares / (pairs * pair_w) + NORM_EPS)
    my_rows = pl.ds(pl.multiple_of(core * half, half), half)

    @pl.loop(0, pairs)
    def _(n):
        scaled = upd[n].astype(jnp.float32) * inv * gain[:, lanes(n * pair_w, pair_w)]
        rows[mine, n, my_rows, :] = scaled.astype(jnp.bfloat16)

    def rows_of(g, at):
        return rows.at[g, :, pl.ds(pl.multiple_of(at * half, half), half), :]

    send("row2", rows_of(mine, core), rows_of(mine, core), (mate(2), core))
    send("row1", rows_of(mine, core), rows_of(mine, core), (mate(1), core))
    send("row0", rows_of(mine, core), rows_of(mine, core), (sp, other))
    crossed("v", 0)
    crossed("v", 1)
    sideways("v", 4)
    across("v", 3)

    def up_dot(g, rels):
        left = jnp.concatenate([rows[g, pair_at(rel)] for rel in rels], axis=1)
        return left

    def up_block(g, rels, fresh):
        seg, x_at = g // 2, g % 2
        start = pl.multiple_of(8 + x_at * tokens, 8)
        left = up_dot(g, rels)

        @pl.loop(0, 2 * ffs // pair_w)
        def _(n):
            cols = lanes(n * pair_w, pair_w)
            part = jnp.zeros((tokens, pair_w), jnp.float32)
            for i, rel in enumerate(rels):
                part = part + jnp.dot(
                    left[:, i * pair_w : (i + 1) * pair_w], wup[rel, :, cols],
                    preferred_element_type=jnp.float32,
                )
            if fresh:
                ups[seg, pl.ds(start, tokens), cols] = part
            else:
                ups[seg, pl.ds(start, tokens), cols] += part

    for kind in "vg":
        from_side(kind, 0)
        from_side(kind, 2)
    arrived("row0", rows_of(mine, other))
    up_block(mine, (0, 2, 1, 3), True)
    across("g", 2)
    arrived("row2", rows_of(place(2), core))
    send("row3", rows_of(place(2), core), rows_of(place(2), core), (mate(1), core))
    send("fwd2", rows_of(place(2), core), rows_of(place(2), core), (sp, other))
    arrived("row1", rows_of(place(1), core))
    send("fwd1", rows_of(place(1), core), rows_of(place(1), core), (sp, other))
    crossed("g", 0)
    crossed("g", 1)
    sideways("g", 4)
    across("g", 3)
    arrived("fwd2", rows_of(place(2), other))
    up_block(place(2), (0, 2, 1, 3), True)
    arrived("fwd1", rows_of(place(1), other))
    up_block(place(1), (0, 2, 1, 3), True)
    locals_[2].wait()
    exchanged("d", 1)
    exchanged("d", 2)
    exchanged("d", 3)
    across("d", 0)
    arrived("row3", rows_of(place(3), core))
    send("fwd3", rows_of(place(3), core), rows_of(place(3), core), (sp, other))
    crossed("v", 2)
    crossed("v", 3)
    sideways("v", 6)
    across("d", 1)
    sideways("d", 0)
    arrived("fwd3", rows_of(place(3), other))
    up_block(place(3), (0, 2, 1, 3), True)
    crossed("g", 2)
    crossed("g", 3)
    sideways("g", 6)
    across("d", 2)
    across("d", 3)

    @pl.loop(0, blocks)
    def _(g):
        up_block(g, (4, 6), False)

    sideways("d", 2)
    for kind in "vg":
        from_side(kind, 4)
        from_side(kind, 6)

    @pl.loop(0, blocks)
    def _(g):
        up_block(g, (5, 7), False)

    span = 2 * tokens
    head, tail = pl.ds(8, 8), pl.ds(span, 8)
    before, after = pl.ds(0, 8), pl.ds(span + 8, 8)
    even = y == 0

    def edge(name, seg_from, rows_from, seg_to, rows_to, device):
        send_at = remote(name, ups.at[seg_from, rows_from, :], ups.at[seg_to, rows_to, :], device)
        return send_at

    @pl.when(even)
    def _():
        edge("h0", 1, head, 0, after, (y_mate, core)).start()
        edge("h1", 0, tail, 0, before, (y_mate, core)).start()
        edge("h2", 1, tail, 1, before, (y_mate, core)).start()

        @pl.when(zh == 1)
        def _():
            edge("h3", 0, head, 1, after, (diag_mate, core)).start()

        @pl.when(zh == 0)
        def _():
            ups[0, before, :] = jnp.zeros((8, 2 * ffs), jnp.float32)

    @pl.when(y == 1)
    def _():
        edge("h0", 0, head, 0, after, (y_mate, core)).start()
        edge("h1", 1, head, 1, after, (y_mate, core)).start()
        edge("h2", 0, tail, 1, before, (y_mate, core)).start()

        @pl.when(zh == 0)
        def _():
            edge("h3", 1, tail, 0, before, (diag_mate, core)).start()

        @pl.when(zh == 1)
        def _():
            ups[1, after, :] = jnp.zeros((8, 2 * ffs), jnp.float32)

    tap_cols = lanes(mine * ffs, ffs)
    tv, tg = taps_v[:, tap_cols], taps_g[:, tap_cols]
    step = 64

    def convolve(window, taps):
        rounded = window.astype(jnp.bfloat16).astype(jnp.float32)
        return (
            rounded[7 : 7 + step] * taps[0:1]
            + rounded[8 : 8 + step] * taps[1:2]
            + rounded[9 : 9 + step] * taps[2:3]
        )

    def hidden_block(i):
        seg, at = i // (span // step), i % (span // step)
        window = pl.ds(pl.multiple_of(at * step, 8), step + 16)
        for n in range(ffs // 128):
            left, right = slice(n * 128, n * 128 + 128), slice(ffs + n * 128, ffs + n * 128 + 128)
            conv_v = convolve(ups[seg, window, left], tv[:, left])
            conv_g = convolve(ups[seg, window, right], tg[:, left])
            value = jax.nn.gelu(conv_g, approximate=True) * conv_v
            hidden[pl.ds(pl.multiple_of(i * step, step), step), left] = value.astype(jnp.bfloat16)

    per = span // step

    @pl.loop(0, 2 * (per - 2))
    def _(i):
        seg = i // (per - 2)
        hidden_block(seg * per + 1 + i % (per - 2))

    @pl.when(even)
    def _():
        edge("h0", 0, head, 0, after, (sp, core)).wait_recv()
        edge("h1", 1, head, 1, after, (sp, core)).wait_recv()
        edge("h2", 0, tail, 1, before, (sp, core)).wait_recv()

        @pl.when(zh == 1)
        def _():
            edge("h3", 1, tail, 0, before, (sp, core)).wait_recv()

    @pl.when(y == 1)
    def _():
        edge("h0", 1, head, 0, after, (sp, core)).wait_recv()
        edge("h1", 0, tail, 0, before, (sp, core)).wait_recv()
        edge("h2", 1, tail, 1, before, (sp, core)).wait_recv()

        @pl.when(zh == 0)
        def _():
            edge("h3", 0, head, 1, after, (sp, core)).wait_recv()

    @pl.loop(0, 4)
    def _(i):
        hidden_block((i // 2) * per + (i % 2) * (per - 1))

    order = [0, 2, 1, 3, 4, 6, 5, 7]

    def down(rel):
        @pl.loop(0, blocks)
        def _(g):
            base = pl.multiple_of(g * tokens, tokens)
            theirs = hidden[pl.ds(pl.multiple_of(base + other * half, half), half), :]
            part_send[rel, g] = jnp.dot(
                theirs, wdown[rel], preferred_element_type=jnp.float32
            ).astype(jnp.bfloat16)

        send(f"part{rel}", part_send.at[rel], part_recv.at[rel], (sp, other))

        @pl.loop(0, blocks)
        def _(g):
            base = pl.multiple_of(g * tokens, tokens)
            ours = hidden[pl.ds(pl.multiple_of(base + core * half, half), half), :]
            part_keep[order.index(rel) % 2, g] = jnp.dot(ours, wdown[rel], preferred_element_type=jnp.float32)

    def merge(rel):
        arrived(f"part{rel}", part_recv.at[rel])
        for at in (2, 3, 1):
            g = place(at)
            both = part_keep[order.index(rel) % 2, g] + part_recv[rel, g].astype(jnp.float32)
            red_send[rel, at - 1] = both.astype(jnp.bfloat16)
            to = rel ^ (at & 2)
            send(f"red{to}{at}", red_send.at[rel, at - 1], red_recv.at[to, at - 1], (mate(at), core))
        fin[rel] = part_keep[order.index(rel) % 2, mine] + part_recv[rel, mine].astype(jnp.float32)

    def close(rel):
        branch = fin[rel]
        for at in (1, 2, 3):
            arrived(f"red{rel}{at}", red_recv.at[rel, at - 1])
            branch = branch + red_recv[rel, at - 1].astype(jnp.float32)
        n = pair_at(rel)
        wide = branch.astype(jnp.bfloat16).astype(jnp.float32)
        out[n] = (upd[n].astype(jnp.float32) + wide).astype(jnp.bfloat16)

    down(0)
    crossed("d", 0)
    crossed("d", 1)
    sideways("d", 4)
    for i, rel in enumerate(order[1:]):
        if rel == 1:
            from_side("d", 0)
        if rel == 3:
            from_side("d", 2)
        if rel == 6:
            crossed("d", 2)
            crossed("d", 3)
            sideways("d", 6)
        if rel == 5:
            from_side("d", 4)
        if rel == 7:
            from_side("d", 6)
        down(rel)
        merge(order[i])
        if i >= 3:
            close(order[i - 3])
    merge(order[-1])
    for rel in order[-4:]:
        close(rel)
    for copy in started:
        copy.wait_send()
    for name in ("h0", "h1", "h2"):
        edge(name, 0, head, 0, after, (sp, core)).wait_send()

    @pl.when((y + zh) == 1)
    def _():
        edge("h3", 0, head, 0, after, (sp, core)).wait_send()


def fused(q_pack, kv_pack, residual, out_weight, norm_gain, value_weight, gate_weight, down_weight,
          conv_value, conv_gate):
    groups, tokens, q_width = q_pack.shape
    half, width = tokens // 2, residual.shape[1]
    depth, ff_here = value_weight.shape
    pair_w = 2 * depth
    pairs = width // pair_w
    ffs = ff_here // groups
    heads = groups * (q_width // HEAD_DIM)
    keys = groups * tokens
    bf16, f32 = jnp.bfloat16, jnp.float32
    vmem, anywhere = pl.BlockSpec(memory_space=pltpu.VMEM), pl.BlockSpec(memory_space=pl.ANY)
    copies = 104
    return pl.pallas_call(
        fused_kernel,
        out_shape=jax.ShapeDtypeStruct((pairs, half, pair_w), bf16),
        in_specs=[vmem, vmem, anywhere, anywhere, vmem, anywhere, anywhere, anywhere, vmem, vmem],
        out_specs=vmem,
        scratch_shapes=[
            pltpu.VMEM((groups, tokens, q_width), bf16),
            pltpu.VMEM((heads, tokens, HEAD_DIM), bf16),
            pltpu.VMEM((4, groups, tokens, 2 * HEAD_DIM), bf16),
            pltpu.VMEM((4, keys, HEAD_DIM), bf16),
            pltpu.VMEM((4, HEAD_DIM, keys), bf16),
            pltpu.VMEM((heads, 1, tokens), f32),
            pltpu.VMEM((heads, 1, tokens), f32),
            pltpu.VMEM((heads, HEAD_DIM, tokens), f32),
            pltpu.VMEM((groups - 1, tokens, q_width), bf16),
            pltpu.VMEM((groups, tokens, q_width), bf16),
            pltpu.VMEM(out_weight.shape, bf16),
            pltpu.VMEM((half, width), bf16),
            pltpu.VMEM((pairs, half, pair_w), bf16),
            pltpu.VMEM((pairs, half, pair_w), bf16),
            pltpu.VMEM((pairs, half, pair_w), bf16),
            pltpu.VMEM((pairs, half, pair_w), bf16),
            pltpu.VMEM((groups, pairs, tokens, pair_w), bf16),
            pltpu.VMEM((pairs, pair_w, 2 * ffs), bf16),
            pltpu.VMEM((pairs, ffs, pair_w), bf16),
            pltpu.VMEM((2, 2 * tokens + 16, 2 * ffs), f32),
            pltpu.VMEM((keys, ffs), bf16),
            pltpu.VMEM((2, groups, half, pair_w), f32),
            pltpu.VMEM((pairs, groups, half, pair_w), bf16),
            pltpu.VMEM((pairs, groups, half, pair_w), bf16),
            pltpu.VMEM((pairs, groups - 1, half, pair_w), bf16),
            pltpu.VMEM((pairs, groups - 1, half, pair_w), bf16),
            pltpu.VMEM((pairs, half, pair_w), f32),
            pltpu.SemaphoreType.DMA((5,)),
            pltpu.SemaphoreType.DMA((copies,)),
            pltpu.SemaphoreType.DMA((copies,)),
        ],
        compiler_params=pltpu.CompilerParams(
            collective_id=0, has_side_effects=True, vmem_limit_bytes=60 * 2**20
        ),
    )(q_pack, kv_pack, residual, out_weight, norm_gain[None, :], value_weight, gate_weight,
      down_weight, conv_value, conv_gate)


def fused_layer(
    query_proj, key_proj, value_proj, q_gain, k_gain, residual, out_weight, norm_gain,
    value_weight, gate_weight, down_weight, conv_value, conv_gate,
):
    tokens = query_proj.shape[0]
    heads_here = query_proj.shape[1] // HEAD_DIM
    kv_here = key_proj.shape[1] // HEAD_DIM
    positions = lax.axis_index("sp") * tokens + jnp.arange(tokens, dtype=jnp.int32)
    queries = grid_rotary(
        rms_norm(query_proj.reshape(tokens, heads_here, HEAD_DIM), q_gain), positions
    ) * HEAD_DIM ** (-0.5)
    queries = queries.astype(jnp.bfloat16)
    keys_rot = grid_rotary(
        rms_norm(key_proj.reshape(tokens, kv_here, HEAD_DIM), k_gain), positions
    ).astype(jnp.bfloat16)
    values = value_proj.reshape(tokens, kv_here, HEAD_DIM)
    q_pack = queries.reshape(tokens, kv_here, -1).transpose(1, 0, 2)
    kv_pack = jnp.concatenate([keys_rot, values], axis=2).transpose(1, 0, 2)
    done = fused(q_pack, kv_pack, residual, out_weight, norm_gain, value_weight, gate_weight,
                 down_weight, conv_value, conv_gate)
    return done.transpose(1, 0, 2).reshape(tokens // 2, -1)


def fits(sp_size, tp_size, arrays):
    tokens, kv_here = arrays[0].shape[0], arrays[1].shape[1] // HEAD_DIM
    depth, ff_here = arrays[8].shape
    return (
        (sp_size, tp_size, kv_here) == (16, 2, 4)
        and depth % 128 == 0
        and ff_here % (kv_here * 128) == 0
        and (2 * ff_here // kv_here) % (2 * depth) == 0
        and tokens % 256 == 0
    )


def layer(*arrays):
    if fits(lax.axis_size("sp"), lax.axis_size("tp"), arrays):
        return fused_layer(*arrays)
    return shards(*arrays)


def solution(mesh):
    return jax.shard_map(
        layer,
        mesh=mesh,
        in_specs=(
            P("sp", "tp"),
            P("sp", "tp"),
            P("sp", "tp"),
            P(),
            P(),
            P("sp", None),
            P("tp", None),
            P(),
            P("sp", "tp"),
            P("sp", "tp"),
            P("tp", "sp"),
            P(None, "tp"),
            P(None, "tp"),
        ),
        out_specs=P(("sp", "tp"), None),
        check_vma=False,
    )
```

```python
import functools
import math

import jax
import jax.numpy as jnp
from jax import lax
from jax.experimental import pallas as pl
from jax.experimental.pallas import tpu as pltpu
from jax.sharding import PartitionSpec as P


HEAD_DIM = 64
GRID_W = 64


NORM_EPS = 1e-06
ROPE_BASE = 10000.0


def rms_norm(block_in, gain_vec):
    values = block_in.astype(jnp.float32)
    inv_rms = lax.rsqrt(jnp.mean(values * values, axis=-1, keepdims=True) + NORM_EPS)
    return values * inv_rms * gain_vec


def rotate_half(values, position):
    full_width = values.shape[-1]
    half_width = full_width // 2
    frequency = ROPE_BASE ** (-jnp.arange(0, full_width, 2, dtype=jnp.float32) / full_width)
    angles = position.astype(jnp.float32)[:, None] * frequency[None, :]
    cosine = jnp.cos(angles)[:, None, :]
    sine_part = jnp.sin(angles)[:, None, :]
    first_half = values[..., :half_width]
    second_half = values[..., half_width:]
    return jnp.concatenate(
        [
            first_half * cosine - second_half * sine_part,
            first_half * sine_part + second_half * cosine,
        ],
        axis=-1,
    )


def grid_rotary(values, positions):
    half_width = values.shape[-1] // 2
    grid_row = positions // GRID_W
    column = positions % GRID_W
    return jnp.concatenate(
        [
            rotate_half(values[..., :half_width], grid_row),
            rotate_half(values[..., half_width:], column),
        ],
        axis=-1,
    )


def exchange_pieces(block_for, place, count, stride, axis_size):
    received = [block_for(place)]
    for hop in range(1, count):
        block = block_for((place + hop) % count)
        received.append(lax.ppermute(block, "sp", shifted(hop, count, stride, axis_size)))
    return received


def in_place_order(received, place):
    count = len(received)
    doubled = (received[::-1] * 2)[: 2 * count - 1]
    size = received[0].shape[0]
    whole = jnp.concatenate(doubled, axis=0)
    return lax.dynamic_slice_in_dim(whole, (count - 1 - place) * size, count * size, 0)


def shifted(hop, count, stride, axis_size):
    pairs = []
    for source in range(axis_size):
        group, rest = source // stride, source % stride
        pairs.append((source, ((group + hop) % count) * stride + rest))
    return pairs


def spread(block, count, stride):
    pieces = [block]
    for flip in range(1, stride):
        pairs = [
            (group * stride + rest, group * stride + (rest ^ flip))
            for group in range(count)
            for rest in range(stride)
        ]
        pieces.append(lax.ppermute(block, "sp", pairs))
    return pieces


def unflip(pieces, rest):
    bit = 1
    while bit < len(pieces):
        chosen = (rest & bit) != 0
        pieces = [
            jnp.where(chosen, pieces[at ^ bit], pieces[at]) for at in range(len(pieces))
        ]
        bit *= 2
    return pieces


def swap_cores(block):
    return lax.ppermute(block, "tp", [(0, 1), (1, 0)])


def attention_kernel(q_ref, k_ref, vt_ref, out_ref, *, span):
    queries = q_ref[...]
    rows, width = queries.shape
    run_max = jnp.full((1, rows), -1e30, jnp.float32)
    run_sum = jnp.zeros((1, rows), jnp.float32)
    run_acc = jnp.zeros((width, rows), jnp.float32)
    for start in range(0, k_ref.shape[0], span):
        scores = lax.dot_general(
            k_ref[start : start + span, :],
            queries,
            (((1,), (1,)), ((), ())),
            preferred_element_type=jnp.float32,
        )
        new_max = jnp.maximum(run_max, jnp.max(scores, axis=0, keepdims=True))
        probs = jnp.exp(scores - new_max)
        shrink = jnp.exp(run_max - new_max)
        run_sum = run_sum * shrink + jnp.sum(probs, axis=0, keepdims=True)
        run_acc = run_acc * shrink + jnp.dot(
            vt_ref[:, start : start + span],
            probs.astype(jnp.bfloat16),
            preferred_element_type=jnp.float32,
        )
        run_max = new_max
    out_ref[...] = (run_acc / run_sum).T.astype(jnp.bfloat16)


def attend(queries, keys, values_t):
    total, width = queries.shape
    key_count = keys.shape[0]
    block = math.gcd(total, 256)
    return pl.pallas_call(
        functools.partial(attention_kernel, span=math.gcd(key_count, 1024)),
        grid=(total // block,),
        out_shape=jax.ShapeDtypeStruct((total, width), jnp.bfloat16),
        in_specs=[
            pl.BlockSpec((block, width), lambda i: (i, 0)),
            pl.BlockSpec((key_count, width), lambda i: (0, 0)),
            pl.BlockSpec((width, key_count), lambda i: (0, 0)),
        ],
        out_specs=pl.BlockSpec((block, width), lambda i: (i, 0)),
        cost_estimate=pl.CostEstimate(
            flops=16 * total * key_count * width,
            bytes_accessed=4 * (total + key_count) * width,
            transcendentals=total * key_count,
        ),
    )(queries, keys, values_t)


def shards(
    query_proj,
    key_proj,
    value_proj,
    q_gain,
    k_gain,
    residual,
    out_weight,
    norm_gain,
    value_weight,
    gate_weight,
    down_weight,
    conv_value,
    conv_gate,
):
    tokens = query_proj.shape[0]
    heads_here = query_proj.shape[1] // HEAD_DIM
    kv_here = key_proj.shape[1] // HEAD_DIM
    group_size = heads_here // kv_here
    sp_size, tp_size = lax.axis_size("sp"), lax.axis_size("tp")
    count = math.gcd(sp_size, 4)
    stride = sp_size // count
    me, core = lax.axis_index("sp"), lax.axis_index("tp")
    place, rest = me // stride, me % stride
    positions = me * tokens + jnp.arange(tokens, dtype=jnp.int32)

    queries = grid_rotary(
        rms_norm(query_proj.reshape(tokens, heads_here, HEAD_DIM), q_gain), positions
    ) * HEAD_DIM ** (-0.5)
    queries = queries.astype(jnp.bfloat16)
    keys_rot = grid_rotary(
        rms_norm(key_proj.reshape(tokens, kv_here, HEAD_DIM), k_gain), positions
    ).astype(jnp.bfloat16)
    values = value_proj.reshape(tokens, kv_here, HEAD_DIM)

    ff_here = value_weight.shape[1]
    depth_here = value_weight.shape[0]
    hidden_here = ff_here // count

    split_heads = count if kv_here % count == 0 else 1
    kv_each = kv_here // split_heads
    packed = jnp.concatenate(
        [queries.reshape(tokens, kv_here, group_size * HEAD_DIM), keys_rot, values], axis=2
    ).transpose(1, 0, 2)
    packed = packed.reshape(split_heads, kv_each, tokens, (group_size + 2) * HEAD_DIM)
    if split_heads > 1:
        got = exchange_pieces(
            lambda at: lax.dynamic_index_in_dim(packed, at, 0, keepdims=False),
            place,
            count,
            stride,
            sp_size,
        )
        got, weights_in = lax.optimization_barrier((got, (value_weight, gate_weight, down_weight)))
    else:
        got, weights_in = [packed[0]], (value_weight, gate_weight, down_weight)
    value_in, gate_in, down_in = weights_in

    q_width = group_size * HEAD_DIM
    kv_mine = jnp.stack([piece[..., q_width:] for piece in got])
    if split_heads > 1:
        kv_all = jnp.stack(spread(kv_mine, count, stride))
    else:
        kv_all = lax.all_gather(kv_mine, "sp", axis=0)
    kv_all = kv_all.transpose(2 + 0, 0, 1, 3, 4).reshape(kv_each, sp_size * tokens, 2 * HEAD_DIM)

    def up_block(at):
        start = at * hidden_here
        return jnp.concatenate(
            [
                lax.dynamic_slice_in_dim(value_in, start, hidden_here, 1),
                lax.dynamic_slice_in_dim(gate_in, start, hidden_here, 1),
            ],
            axis=1,
        )

    def down_block(at):
        return lax.dynamic_slice_in_dim(down_in, at * hidden_here, hidden_here, 0)

    up_got = exchange_pieces(up_block, place, count, stride, sp_size)
    up_pieces = spread(in_place_order(up_got, place), count, stride)
    columns_here = down_weight.shape[1]
    down_got = exchange_pieces(down_block, place, count, stride, sp_size)
    down_cols = in_place_order(down_got, place).reshape(count, hidden_here, columns_here)
    down_cols = jnp.concatenate([down_cols[at] for at in range(count)], axis=1)
    down_pieces = spread(down_cols, count, stride)

    q_pieces = [piece[..., :q_width] for piece in got]
    per_head = []
    for kv_at in range(kv_each):
        keys_h = kv_all[kv_at, :, :HEAD_DIM]
        values_t = kv_all[kv_at, :, HEAD_DIM:].T
        per_group = []
        for group_at in range(group_size):
            columns = slice(group_at * HEAD_DIM, (group_at + 1) * HEAD_DIM)
            q_here = jnp.concatenate([piece[kv_at, :, columns] for piece in q_pieces], axis=0)
            per_group.append(attend(q_here, keys_h, values_t))
        per_head.append(jnp.concatenate(per_group, axis=1))
    done = jnp.concatenate(per_head, axis=1).reshape(len(got), tokens, -1)
    if split_heads > 1:
        back = [done[0]]
        for hop in range(1, count):
            back.append(lax.ppermute(done[hop], "sp", shifted(-hop, count, stride, sp_size)))
        attended = jnp.roll(jnp.stack(back), place, axis=0).transpose(1, 0, 2)
        attended = attended.reshape(tokens, heads_here * HEAD_DIM)
    else:
        attended = done[0]

    row_share = tokens // tp_size
    residual_mine = lax.dynamic_slice_in_dim(residual, core * row_share, row_share, 0)
    if tp_size == 2:
        weight_other = swap_cores(out_weight)
        halves = attended.reshape(2, row_share, heads_here * HEAD_DIM)
        rows_mine = lax.dynamic_index_in_dim(halves, core, 0, keepdims=False)
        rows_other = swap_cores(lax.dynamic_index_in_dim(halves, 1 - core, 0, keepdims=False))
        mix_mine = jnp.dot(rows_mine, out_weight, preferred_element_type=jnp.float32)
        mix_other = jnp.dot(rows_other, weight_other, preferred_element_type=jnp.float32)
        mix_out = (
            mix_mine.astype(jnp.bfloat16).astype(jnp.float32)
            + mix_other.astype(jnp.bfloat16).astype(jnp.float32)
        ).astype(jnp.bfloat16)
    else:
        mix_out = lax.psum_scatter(
            jnp.dot(attended, out_weight, preferred_element_type=jnp.float32).astype(jnp.bfloat16),
            "tp",
            scatter_dimension=0,
            tiled=True,
        )
    updated = (residual_mine.astype(jnp.float32) + mix_out.astype(jnp.float32)).astype(jnp.bfloat16)
    normed = rms_norm(updated, norm_gain).astype(jnp.bfloat16)
    width = normed.shape[1]
    normed = jnp.stack(
        [
            jnp.concatenate(
                [
                    normed[:, (at * stride + flip) * depth_here :][:, :depth_here]
                    for at in range(count)
                ],
                axis=1,
            )
            for flip in range(stride)
        ]
    )

    ups = []
    for hop in range(count):
        rows = normed
        if hop:
            rows = lax.ppermute(normed, "sp", shifted(hop, count, stride, sp_size))
        if tp_size == 2:
            other = swap_cores(rows)
            rows = jnp.concatenate(
                [jnp.where(core == 0, rows, other), jnp.where(core == 0, other, rows)], axis=1
            )
        else:
            rows = lax.all_gather(rows, "tp", axis=1, tiled=True)
        total = 0.0
        for flip in range(stride):
            part = lax.dynamic_index_in_dim(rows, rest ^ flip, 0, keepdims=False)
            total = total + jnp.dot(part, up_pieces[flip], preferred_element_type=jnp.float32)
        ups.append(total.astype(jnp.bfloat16))
    ups = jnp.stack(ups)

    forward = [
        (group * stride + at, group * stride + (at + 1) % stride)
        for group in range(count)
        for at in range(stride)
    ]
    backward = [(target, source) for source, target in forward]
    before = lax.ppermute(ups[:, -1], "sp", forward)
    after = lax.ppermute(ups[:, 0], "sp", backward)
    hops = jnp.arange(count)
    block_at = (place - hops) % count
    no_before = (rest == 0) & (block_at == 0)
    no_after = (rest == stride - 1) & (block_at == count - 1)
    before = jnp.where(rest == 0, jnp.roll(before, -1, axis=0), before)
    after = jnp.where(rest == stride - 1, jnp.roll(after, 1, axis=0), after)
    before = jnp.where(no_before[:, None], 0, before)
    after = jnp.where(no_after[:, None], 0, after)
    padded = jnp.concatenate([before[:, None], ups, after[:, None]], axis=1).astype(jnp.float32)
    taps = jnp.concatenate(
        [
            lax.dynamic_slice_in_dim(conv_value, place * hidden_here, hidden_here, 1),
            lax.dynamic_slice_in_dim(conv_gate, place * hidden_here, hidden_here, 1),
        ],
        axis=1,
    )
    conv = padded[:, :-2] * taps[0] + padded[:, 1:-1] * taps[1] + padded[:, 2:] * taps[2]
    hidden = (
        jax.nn.gelu(conv[..., hidden_here:], approximate=True) * conv[..., :hidden_here]
    ).astype(jnp.bfloat16)

    down_all = jnp.concatenate(down_pieces, axis=1)
    branch = 0.0
    for hop in list(range(1, count)) + [0]:
        partial = jnp.dot(hidden[hop], down_all, preferred_element_type=jnp.float32)
        if tp_size == 2:
            partial = partial.reshape(2, row_share, width)
            mine = lax.dynamic_index_in_dim(partial, core, 0, keepdims=False)
            theirs = lax.dynamic_index_in_dim(partial, 1 - core, 0, keepdims=False)
            other = swap_cores(theirs.astype(jnp.bfloat16))
            mine = mine + other.astype(jnp.float32)
        else:
            mine = lax.psum_scatter(
                partial.astype(jnp.bfloat16), "tp", scatter_dimension=0, tiled=True
            )
        if hop:
            mine = lax.ppermute(
                mine.astype(jnp.bfloat16), "sp", shifted(-hop, count, stride, sp_size)
            )
        branch = branch + mine.astype(jnp.float32)
    branch = branch.astype(jnp.bfloat16)
    span = count * columns_here
    pieces = unflip([branch[:, at * span : (at + 1) * span] for at in range(stride)], rest)
    branch = jnp.concatenate(
        [
            pieces[at][:, group * columns_here : (group + 1) * columns_here]
            for group in range(count)
            for at in range(stride)
        ],
        axis=1,
    )
    return (updated.astype(jnp.float32) + branch.astype(jnp.float32)).astype(jnp.bfloat16)


def fused_kernel(
    q_in, kv_in, res_in, wo_in, gain, wv_in, wg_in, wd_in, taps_v, taps_g, out,
    qraw, qhead, kvbuf, kbuf, vbuf, top, total, acc, att_send, att_all, wo, res, mix_send, mix_recv,
    own_mix, upd, rows, wup, wdown, ups, hidden, part_keep, part_send, part_recv, red_send,
    red_recv, fin, local_sem, send_sem, recv_sem,
):
    sp, core = lax.axis_index("sp"), lax.axis_index("tp")
    x, y, zl, zh = sp % 2, (sp // 2) % 2, (sp // 4) % 2, sp // 8
    fx, fy, fl, fh = 1 - 2 * x, 1 - 2 * y, 1 - 2 * zl, 1 - 2 * zh
    depth = wv_in.shape[0]
    ffs = wdown.shape[1]
    pairs, half, pair_w = upd.shape
    tokens = 2 * half
    other = 1 - core

    def xs(flip):
        return x + fx * flip

    def mate(at):
        return sp + fx * (at % 2) + 4 * fl * (at // 2)

    def place(at):
        return xs(at % 2) + 2 * (zl + fl * (at // 2))

    mine = place(0)
    y_mate, z_mate = sp + 2 * fy, sp + 8 * fh
    diag_mate = sp + 2 * fy + 8 * fh

    def pair_at(rel):
        return (y + fy * (rel % 2)) + 2 * (zl + fl * ((rel // 2) % 2)) + 4 * (zh + fh * (rel // 4))

    ids = {}
    started = []

    def remote(name, src, dst, device):
        at = ids.setdefault(name, len(ids))
        assert at < send_sem.shape[0], len(ids)
        return pltpu.make_async_remote_copy(
            src_ref=src, dst_ref=dst, send_sem=send_sem.at[at], recv_sem=recv_sem.at[at],
            device_id=device, device_id_type=pl.DeviceIdType.MESH,
        )

    def send(name, src, dst, device):
        copy = remote(name, src, dst, device)
        copy.start()
        started.append(copy)

    def arrived(name, dst):
        remote(name, dst, dst, (sp, core)).wait_recv()

    def lanes(start, size):
        return pl.ds(pl.multiple_of(start, 128), size)

    barrier = pltpu.get_barrier_semaphore()
    partners = [(sp, other)] + [(mate(at), core) for at in (1, 2, 3)]
    partners += [(y_mate, core), (z_mate, core), (diag_mate, core)]
    for device in partners:
        pl.semaphore_signal(barrier, inc=1, device_id=device, device_id_type=pl.DeviceIdType.MESH)
    pl.semaphore_wait(barrier, len(partners))

    def piece(kind, rel, x_at):
        start = pl.multiple_of(x_at * depth, depth)
        if kind == "v":
            return wup.at[rel, pl.ds(start, depth), pl.ds(0, ffs)]
        if kind == "g":
            return wup.at[rel, pl.ds(start, depth), pl.ds(ffs, ffs)]
        return wdown.at[rel, :, pl.ds(start, depth)]

    def whole(kind, rel):
        if kind == "v":
            return wup.at[rel, :, pl.ds(0, ffs)]
        if kind == "g":
            return wup.at[rel, :, pl.ds(ffs, ffs)]
        return wdown.at[rel]

    def shard(kind, at):
        if kind == "d":
            return wd_in.at[pl.ds(pl.multiple_of(place(at) * ffs, 128), ffs), :]
        return (wv_in if kind == "v" else wg_in).at[:, lanes(place(at) * ffs, ffs)]

    def launch(name, src, dst, device, where):
        fresh = name not in ids
        copy = remote(name, src, dst, device)
        if where is None:
            copy.start()
        else:
            pl.when(where)(copy.start)
        if fresh:
            started.append(copy)

    def exchange(kind, at, where=None):
        dst = piece(kind, 2 * (at // 2), x)
        launch(f"w1{kind}{at}", shard(kind, at), dst, (mate(at), core), where)

    def exchanged(kind, at):
        arrived(f"w1{kind}{at}", piece(kind, 2 * (at // 2), xs(at % 2)))

    inner, outer = zl != zh, zl == zh

    def across(kind, at, where=None):
        src = piece(kind, 2 * (at // 2), xs(at % 2)) if at else shard(kind, 0)
        dst = piece(kind, 2 * (at // 2) + 4, xs(at % 2))
        launch(f"wz{kind}{at}", src, dst, (z_mate, core), where)

    def crossed(kind, at):
        arrived(f"wz{kind}{at}", piece(kind, 2 * (at // 2) + 4, xs(at % 2)))

    def sideways(kind, rel):
        send(f"wy{kind}{rel}", whole(kind, rel), whole(kind, rel + 1), (y_mate, core))

    def sideways_half(kind, at):
        src = piece(kind, 0, xs(at)) if at else shard(kind, 0)
        send(f"wy{kind}h{at}", src, piece(kind, 1, xs(at)), (y_mate, core))

    def from_side(kind, rel):
        if rel or kind == "d":
            arrived(f"wy{kind}{rel}", whole(kind, rel + 1))
        else:
            arrived(f"wy{kind}h0", piece(kind, 1, x))
            arrived(f"wy{kind}h1", piece(kind, 1, xs(1)))

    for at in (2, 3, 1):
        send(f"kv{at}", kv_in.at[place(at)], kvbuf.at[0, mine], (mate(at), core))
    for at in (2, 3, 1):
        send(f"q{at}", q_in.at[place(at)], qraw.at[mine], (mate(at), core))
    locals_ = [
        pltpu.make_async_copy(shard(kind, 0), piece(kind, 0, x), local_sem.at[n])
        for n, kind in enumerate("vgd")
    ]
    locals_.append(pltpu.make_async_copy(wo_in, wo, local_sem.at[3]))
    locals_.append(
        pltpu.make_async_copy(
            res_in.at[pl.ds(pl.multiple_of(core * half, half), half), :], res, local_sem.at[4]
        )
    )
    for copy in locals_:
        copy.start()
    qraw[mine] = q_in[mine]
    kvbuf[0, mine] = kv_in[mine]
    top[...] = jnp.full(top.shape, -1e30, jnp.float32)
    total[...] = jnp.zeros(total.shape, jnp.float32)
    acc[...] = jnp.zeros(acc.shape, jnp.float32)
    for at in (1, 2, 3):
        arrived(f"kv{at}", kvbuf.at[0, place(at)])
    send("kvz", kvbuf.at[0], kvbuf.at[2], (z_mate, core))
    send("kvy", kvbuf.at[0], kvbuf.at[1], (y_mate, core))
    across("v", 0)
    sideways_half("v", 0)
    for at in (1, 2, 3):
        exchange("v", at)
    sideways_half("g", 0)
    for at in (1, 2, 3):
        arrived(f"q{at}", qraw.at[place(at)])
    for at in (2, 3, 1):
        exchange("g", at)
    width = HEAD_DIM
    group = qraw.shape[2] // width
    blocks = qraw.shape[0]

    @pl.loop(0, blocks)
    def _(b):
        for a in range(group):
            qhead[b * group + a] = qraw[b][:, a * width : (a + 1) * width]

    def unpack(t):
        @pl.loop(0, blocks)
        def _(b):
            start = pl.multiple_of(b * tokens, tokens)
            pair = kvbuf[t, b]
            kbuf[t, pl.ds(start, tokens), :] = pair[:, :width]
            vbuf[t, :, pl.ds(start, tokens)] = pair[:, width:].T

    def attend_block(t, h):
        scores = lax.dot_general(
            kbuf[t], qhead[h], (((1,), (1,)), ((), ())), preferred_element_type=jnp.float32
        )
        old = top[h]
        new = jnp.maximum(old, jnp.max(scores, axis=0, keepdims=True))
        probs = jnp.exp(scores - new)
        shrink = jnp.exp(old - new)
        total[h] = total[h] * shrink + jnp.sum(probs, axis=0, keepdims=True)
        acc[h] = acc[h] * shrink + jnp.dot(
            vbuf[t], probs.astype(jnp.bfloat16), preferred_element_type=jnp.float32
        )
        top[h] = new

    def attend_some(t, lo, hi):
        @pl.loop(lo, hi)
        def _(h):
            attend_block(t, h)

    heads = blocks * group
    unpack(0)
    attend_some(0, 0, heads // 2)
    for copy in locals_[:3]:
        copy.wait()
    exchanged("v", 1)
    across("v", 1)
    sideways_half("v", 1)
    across("g", 0)
    attend_some(0, heads // 2, heads)
    arrived("kvy", kvbuf.at[1])
    unpack(1)
    attend_some(1, 0, heads // 2)
    exchanged("g", 1)
    across("g", 1)
    sideways_half("g", 1)
    attend_some(1, heads // 2, heads)
    arrived("kvz", kvbuf.at[2])
    send("kvd", kvbuf.at[2], kvbuf.at[3], (y_mate, core))
    unpack(2)
    attend_some(2, 0, heads // 2)
    exchanged("v", 2)
    exchanged("v", 3)
    sideways("v", 2)
    across("v", 2)
    across("v", 3)
    attend_some(2, heads // 2, heads)
    arrived("kvd", kvbuf.at[3])
    unpack(3)

    def finish(block):
        first = block * group
        pieces = [acc[first + a] / total[first + a] for a in range(group)]
        return jnp.concatenate(pieces, axis=0).T.astype(jnp.bfloat16)

    for at in (2, 3, 1, 0):
        block = place(at)
        attend_some(3, block * group, block * group + group)
        if at:
            att_send[at - 1] = finish(block)
            send(f"att{at}", att_send.at[at - 1], att_all.at[mine], (mate(at), core))
        else:
            att_all[mine] = finish(block)
    exchanged("g", 2)
    exchanged("g", 3)
    sideways("g", 2)
    exchange("d", 1)
    for copy in locals_[3:]:
        copy.wait()
    for at in (1, 2, 3):
        arrived(f"att{at}", att_all.at[place(at)])
    crossed("v", 0)
    crossed("v", 1)
    sideways("v", 4)

    def project(n, rows_at):
        start = pl.multiple_of(rows_at * half, half)
        left = jnp.concatenate([att_all[b, pl.ds(start, half), :] for b in range(blocks)], axis=1)
        return jnp.dot(left, wo[:, lanes(n * pair_w, pair_w)], preferred_element_type=jnp.float32)

    @pl.loop(0, pairs)
    def _(n):
        mix_send[n] = project(n, other).astype(jnp.bfloat16)

    send("mix", mix_send, mix_recv, (sp, other))

    @pl.loop(0, pairs)
    def _(n):
        own_mix[n] = project(n, core).astype(jnp.bfloat16)

    arrived("mix", mix_recv)

    def update(n, squares):
        mixed = own_mix[n].astype(jnp.float32) + mix_recv[n].astype(jnp.float32)
        mixed = mixed.astype(jnp.bfloat16).astype(jnp.float32)
        held = res[:, lanes(n * pair_w, pair_w)].astype(jnp.float32)
        new = (held + mixed).astype(jnp.bfloat16)
        upd[n] = new
        wide = new.astype(jnp.float32)
        return squares + jnp.sum(wide * wide, axis=1, keepdims=True)

    squares = lax.fori_loop(0, pairs, update, jnp.zeros((half, 1), jnp.float32))
    inv = lax.rsqrt(squares / (pairs * pair_w) + NORM_EPS)
    my_rows = pl.ds(pl.multiple_of(core * half, half), half)

    @pl.loop(0, pairs)
    def _(n):
        scaled = upd[n].astype(jnp.float32) * inv * gain[:, lanes(n * pair_w, pair_w)]
        rows[mine, n, my_rows, :] = scaled.astype(jnp.bfloat16)

    def rows_of(g, at):
        return rows.at[g, :, pl.ds(pl.multiple_of(at * half, half), half), :]

    send("row2", rows_of(mine, core), rows_of(mine, core), (mate(2), core))
    send("row1", rows_of(mine, core), rows_of(mine, core), (mate(1), core))
    send("row0", rows_of(mine, core), rows_of(mine, core), (sp, other))
    across("g", 2, outer)
    across("g", 3, outer)
    for at in (2, 3):
        exchange("d", at, outer)

    def up_dot(g, rels):
        left = jnp.concatenate([rows[g, pair_at(rel)] for rel in rels], axis=1)
        return left

    def up_block(g, rels, fresh):
        up_inner(g, rels, fresh)

    def up_inner(g, rels, fresh):
        seg, x_at = g // 2, g % 2
        start = pl.multiple_of(8 + x_at * tokens, 8)
        left = up_dot(g, rels)

        @pl.loop(0, 2 * ffs // pair_w)
        def _(n):
            cols = lanes(n * pair_w, pair_w)
            part = jnp.zeros((tokens, pair_w), jnp.float32)
            for i, rel in enumerate(rels):
                part = part + jnp.dot(
                    left[:, i * pair_w : (i + 1) * pair_w], wup[rel, :, cols],
                    preferred_element_type=jnp.float32,
                )
            if fresh:
                ups[seg, pl.ds(start, tokens), cols] = part
            else:
                ups[seg, pl.ds(start, tokens), cols] += part

    for kind in "vg":
        from_side(kind, 0)
        from_side(kind, 2)
    arrived("row0", rows_of(mine, other))
    up_block(mine, (0, 2, 1, 3), True)
    crossed("g", 0)
    crossed("g", 1)
    sideways("g", 4)
    arrived("row2", rows_of(place(2), core))
    send("row3", rows_of(place(2), core), rows_of(place(2), core), (mate(1), core))
    send("fwd2", rows_of(place(2), core), rows_of(place(2), core), (sp, other))
    exchanged("d", 1)
    sideways("d", 0)
    arrived("row1", rows_of(place(1), core))
    send("fwd1", rows_of(place(1), core), rows_of(place(1), core), (sp, other))
    across("d", 0, outer)
    across("d", 1, outer)
    arrived("fwd2", rows_of(place(2), other))
    up_block(place(2), (0, 2, 1, 3), True)
    across("g", 2, inner)
    across("g", 3, inner)
    arrived("fwd1", rows_of(place(1), other))
    up_block(place(1), (0, 2, 1, 3), True)
    for at in (2, 3):
        exchange("d", at, inner)
    crossed("v", 2)
    crossed("v", 3)
    sideways("v", 6)
    arrived("row3", rows_of(place(3), core))
    send("fwd3", rows_of(place(3), core), rows_of(place(3), core), (sp, other))
    across("d", 0, inner)
    across("d", 1, inner)
    arrived("fwd3", rows_of(place(3), other))
    up_block(place(3), (0, 2, 1, 3), True)
    crossed("g", 2)
    crossed("g", 3)
    sideways("g", 6)

    @pl.loop(0, blocks)
    def _(g):
        up_block(g, (4, 6), False)

    exchanged("d", 2)
    exchanged("d", 3)
    across("d", 2)
    across("d", 3)
    sideways("d", 2)
    for kind in "vg":
        from_side(kind, 4)
        from_side(kind, 6)

    @pl.loop(0, blocks)
    def _(g):
        up_block(g, (5, 7), False)

    span = 2 * tokens
    head, tail = pl.ds(8, 8), pl.ds(span, 8)
    before, after = pl.ds(0, 8), pl.ds(span + 8, 8)
    even = y == 0

    def edge(name, seg_from, rows_from, seg_to, rows_to, device):
        send_at = remote(name, ups.at[seg_from, rows_from, :], ups.at[seg_to, rows_to, :], device)
        return send_at

    @pl.when(even)
    def _():
        edge("h0", 1, head, 0, after, (y_mate, core)).start()
        edge("h1", 0, tail, 0, before, (y_mate, core)).start()
        edge("h2", 1, tail, 1, before, (y_mate, core)).start()

        @pl.when(zh == 1)
        def _():
            edge("h3", 0, head, 1, after, (diag_mate, core)).start()

        @pl.when(zh == 0)
        def _():
            ups[0, before, :] = jnp.zeros((8, 2 * ffs), jnp.float32)

    @pl.when(y == 1)
    def _():
        edge("h0", 0, head, 0, after, (y_mate, core)).start()
        edge("h1", 1, head, 1, after, (y_mate, core)).start()
        edge("h2", 0, tail, 1, before, (y_mate, core)).start()

        @pl.when(zh == 0)
        def _():
            edge("h3", 1, tail, 0, before, (diag_mate, core)).start()

        @pl.when(zh == 1)
        def _():
            ups[1, after, :] = jnp.zeros((8, 2 * ffs), jnp.float32)

    tap_cols = lanes(mine * ffs, ffs)
    tv, tg = taps_v[:, tap_cols], taps_g[:, tap_cols]
    step = 64

    def convolve(window, taps):
        rounded = window.astype(jnp.bfloat16).astype(jnp.float32)
        return (
            rounded[7 : 7 + step] * taps[0:1]
            + rounded[8 : 8 + step] * taps[1:2]
            + rounded[9 : 9 + step] * taps[2:3]
        )

    def hidden_block(i):
        seg, at = i // (span // step), i % (span // step)
        window = pl.ds(pl.multiple_of(at * step, 8), step + 16)
        for n in range(ffs // 128):
            left, right = slice(n * 128, n * 128 + 128), slice(ffs + n * 128, ffs + n * 128 + 128)
            conv_v = convolve(ups[seg, window, left], tv[:, left])
            conv_g = convolve(ups[seg, window, right], tg[:, left])
            value = jax.nn.gelu(conv_g, approximate=True) * conv_v
            block, at_row = i // (tokens // step), (i % (tokens // step)) * step
            to = (at_row // half) * blocks * half + block * half + at_row % half
            hidden[pl.ds(pl.multiple_of(to, step), step), left] = value.astype(jnp.bfloat16)

    per = span // step

    @pl.loop(0, 2 * (per - 2))
    def _(i):
        seg = i // (per - 2)
        hidden_block(seg * per + 1 + i % (per - 2))

    @pl.when(even)
    def _():
        edge("h0", 0, head, 0, after, (sp, core)).wait_recv()
        edge("h1", 1, head, 1, after, (sp, core)).wait_recv()
        edge("h2", 0, tail, 1, before, (sp, core)).wait_recv()

        @pl.when(zh == 1)
        def _():
            edge("h3", 1, tail, 0, before, (sp, core)).wait_recv()

    @pl.when(y == 1)
    def _():
        edge("h0", 1, head, 0, after, (sp, core)).wait_recv()
        edge("h1", 0, tail, 0, before, (sp, core)).wait_recv()
        edge("h2", 1, tail, 1, before, (sp, core)).wait_recv()

        @pl.when(zh == 0)
        def _():
            edge("h3", 0, head, 1, after, (sp, core)).wait_recv()

    crossed("d", 0)
    crossed("d", 1)
    sideways("d", 4)

    @pl.loop(0, 4)
    def _(i):
        hidden_block((i // 2) * per + (i % 2) * (per - 1))

    order = [0, 2, 1, 3, 4, 6, 5, 7]
    straight = order[-2:]

    def down(rel):
        def product(at):
            left = hidden[pl.ds(pl.multiple_of(at * blocks * half, half), blocks * half), :]
            whole_part = jnp.dot(left, wdown[rel], preferred_element_type=jnp.float32)
            return whole_part.reshape(blocks, half, pair_w)

        part_send[rel] = product(other).astype(jnp.bfloat16)
        send(f"part{rel}", part_send.at[rel], part_recv.at[rel], (sp, other))
        part_keep[order.index(rel) % 2] = product(core)

    def merge(rel):
        arrived(f"part{rel}", part_recv.at[rel])

        def both(at):
            g = place(at)
            return part_keep[order.index(rel) % 2, g] + part_recv[rel, g].astype(jnp.float32)

        if rel in straight:
            for at in (2, 3, 1):
                red_send[rel, at - 1] = both(at).astype(jnp.bfloat16)
                to = across_rel(rel, at)
                send(f"red{to}{at}", red_send.at[rel, at - 1], red_recv.at[to, at - 1],
                     (mate(at), core))
            fin[rel, 0] = both(0)
            return
        first, second = ways(rel)
        for i, at in enumerate((first, 3)):
            red_send[rel, i] = both(at).astype(jnp.bfloat16)
        to = across_rel(rel, first)
        send(f"reda{to}", red_send.at[rel, pl.ds(0, 2)], red_recv.at[to, pl.ds(0, 2)],
             (mate(first), core))
        fin[rel, 0] = both(0)
        fin[rel, 1] = both(second)

    def ways(rel):
        return (1, 2) if rel < 4 and rel % 2 == 0 else (2, 1)

    def across_rel(rel, at):
        return rel ^ (at & 2)

    def pass_on(rel):
        second = ways(rel)[1]
        arrived(f"reda{rel}", red_recv.at[rel, pl.ds(0, 2)])
        red_send[rel, 2] = (fin[rel, 1] + red_recv[rel, 1].astype(jnp.float32)).astype(jnp.bfloat16)
        to = across_rel(rel, second)
        send(f"redb{to}", red_send.at[rel, 2], red_recv.at[to, 2], (mate(second), core))

    def close(rel):
        branch = fin[rel, 0]
        if rel in straight:
            for at in (1, 2, 3):
                arrived(f"red{rel}{at}", red_recv.at[rel, at - 1])
                branch = branch + red_recv[rel, at - 1].astype(jnp.float32)
        else:
            arrived(f"redb{rel}", red_recv.at[rel, 2])
            branch = branch + red_recv[rel, 0].astype(jnp.float32)
            branch = branch + red_recv[rel, 2].astype(jnp.float32)
        n = pair_at(rel)
        wide = branch.astype(jnp.bfloat16).astype(jnp.float32)
        new = (upd[n].astype(jnp.float32) + wide).astype(jnp.bfloat16)
        out[:, lanes(n * pair_w, pair_w)] = new

    down(0)
    for i, rel in enumerate(order[1:]):
        if rel == 1:
            from_side("d", 0)
        if rel == 3:
            from_side("d", 2)
        if rel == 4:
            crossed("d", 2)
            crossed("d", 3)
            sideways("d", 6)
        if rel == 5:
            from_side("d", 4)
        if rel == 7:
            from_side("d", 6)
        down(rel)
        merge(order[i])
        if i >= 2:
            pass_on(order[i - 2])
    merge(order[-1])
    pass_on(order[-3])
    for rel in order:
        close(rel)
    for copy in started:
        copy.wait_send()
    for name in ("h0", "h1", "h2"):
        edge(name, 0, head, 0, after, (sp, core)).wait_send()

    @pl.when((y + zh) == 1)
    def _():
        edge("h3", 0, head, 0, after, (sp, core)).wait_send()


def fused(q_pack, kv_pack, residual, out_weight, norm_gain, value_weight, gate_weight, down_weight,
          conv_value, conv_gate):
    groups, tokens, q_width = q_pack.shape
    half, width = tokens // 2, residual.shape[1]
    depth, ff_here = value_weight.shape
    pair_w = 2 * depth
    pairs = width // pair_w
    ffs = ff_here // groups
    heads = groups * (q_width // HEAD_DIM)
    keys = groups * tokens
    bf16, f32 = jnp.bfloat16, jnp.float32
    vmem, anywhere = pl.BlockSpec(memory_space=pltpu.VMEM), pl.BlockSpec(memory_space=pl.ANY)
    copies = 104
    return pl.pallas_call(
        fused_kernel,
        out_shape=jax.ShapeDtypeStruct((half, width), bf16),
        in_specs=[vmem, vmem, anywhere, anywhere, vmem, anywhere, anywhere, anywhere, vmem, vmem],
        out_specs=vmem,
        scratch_shapes=[
            pltpu.VMEM((groups, tokens, q_width), bf16),
            pltpu.VMEM((heads, tokens, HEAD_DIM), bf16),
            pltpu.VMEM((4, groups, tokens, 2 * HEAD_DIM), bf16),
            pltpu.VMEM((4, keys, HEAD_DIM), bf16),
            pltpu.VMEM((4, HEAD_DIM, keys), bf16),
            pltpu.VMEM((heads, 1, tokens), f32),
            pltpu.VMEM((heads, 1, tokens), f32),
            pltpu.VMEM((heads, HEAD_DIM, tokens), f32),
            pltpu.VMEM((groups - 1, tokens, q_width), bf16),
            pltpu.VMEM((groups, tokens, q_width), bf16),
            pltpu.VMEM(out_weight.shape, bf16),
            pltpu.VMEM((half, width), bf16),
            pltpu.VMEM((pairs, half, pair_w), bf16),
            pltpu.VMEM((pairs, half, pair_w), bf16),
            pltpu.VMEM((pairs, half, pair_w), bf16),
            pltpu.VMEM((pairs, half, pair_w), bf16),
            pltpu.VMEM((groups, pairs, tokens, pair_w), bf16),
            pltpu.VMEM((pairs, pair_w, 2 * ffs), bf16),
            pltpu.VMEM((pairs, ffs, pair_w), bf16),
            pltpu.VMEM((2, 2 * tokens + 16, 2 * ffs), f32),
            pltpu.VMEM((keys, ffs), bf16),
            pltpu.VMEM((2, groups, half, pair_w), f32),
            pltpu.VMEM((pairs, groups, half, pair_w), bf16),
            pltpu.VMEM((pairs, groups, half, pair_w), bf16),
            pltpu.VMEM((pairs, groups - 1, half, pair_w), bf16),
            pltpu.VMEM((pairs, groups - 1, half, pair_w), bf16),
            pltpu.VMEM((pairs, 2, half, pair_w), f32),
            pltpu.SemaphoreType.DMA((5,)),
            pltpu.SemaphoreType.DMA((copies,)),
            pltpu.SemaphoreType.DMA((copies,)),
        ],
        compiler_params=pltpu.CompilerParams(
            collective_id=0, has_side_effects=True, vmem_limit_bytes=60 * 2**20
        ),
    )(q_pack, kv_pack, residual, out_weight, norm_gain[None, :], value_weight, gate_weight,
      down_weight, conv_value, conv_gate)


def fused_layer(
    query_proj, key_proj, value_proj, q_gain, k_gain, residual, out_weight, norm_gain,
    value_weight, gate_weight, down_weight, conv_value, conv_gate,
):
    tokens = query_proj.shape[0]
    heads_here = query_proj.shape[1] // HEAD_DIM
    kv_here = key_proj.shape[1] // HEAD_DIM
    positions = lax.axis_index("sp") * tokens + jnp.arange(tokens, dtype=jnp.int32)
    queries = grid_rotary(
        rms_norm(query_proj.reshape(tokens, heads_here, HEAD_DIM), q_gain), positions
    ) * HEAD_DIM ** (-0.5)
    queries = queries.astype(jnp.bfloat16)
    keys_rot = grid_rotary(
        rms_norm(key_proj.reshape(tokens, kv_here, HEAD_DIM), k_gain), positions
    ).astype(jnp.bfloat16)
    values = value_proj.reshape(tokens, kv_here, HEAD_DIM)
    q_pack = queries.reshape(tokens, kv_here, -1).transpose(1, 0, 2)
    kv_pack = jnp.concatenate([keys_rot, values], axis=2).transpose(1, 0, 2)
    return fused(q_pack, kv_pack, residual, out_weight, norm_gain, value_weight, gate_weight,
                 down_weight, conv_value, conv_gate)


def fits(sp_size, tp_size, arrays):
    tokens, kv_here = arrays[0].shape[0], arrays[1].shape[1] // HEAD_DIM
    depth, ff_here = arrays[8].shape
    return (
        (sp_size, tp_size, kv_here) == (16, 2, 4)
        and depth % 128 == 0
        and ff_here % (kv_here * 128) == 0
        and (2 * ff_here // kv_here) % (2 * depth) == 0
        and tokens % 256 == 0
    )


def layer(*arrays):
    if fits(lax.axis_size("sp"), lax.axis_size("tp"), arrays):
        return fused_layer(*arrays)
    return shards(*arrays)


def solution(mesh):
    return jax.shard_map(
        layer,
        mesh=mesh,
        in_specs=(
            P("sp", "tp"),
            P("sp", "tp"),
            P("sp", "tp"),
            P(),
            P(),
            P("sp", None),
            P("tp", None),
            P(),
            P("sp", "tp"),
            P("sp", "tp"),
            P("tp", "sp"),
            P(None, "tp"),
            P(None, "tp"),
        ),
        out_specs=P(("sp", "tp"), None),
        check_vma=False,
    )
```

```python
import functools
import math

import jax
import jax.numpy as jnp
import numpy as np
from jax import lax
from jax.experimental import pallas as pl
from jax.experimental.pallas import tpu as pltpu
from jax.sharding import PartitionSpec as P


HEAD_DIM = 64
GRID_W = 64


NORM_EPS = 1e-06
ROPE_BASE = 10000.0


def rms_norm(block_in, gain_vec):
    values = block_in.astype(jnp.float32)
    inv_rms = lax.rsqrt(jnp.mean(values * values, axis=-1, keepdims=True) + NORM_EPS)
    return values * inv_rms * gain_vec


def rotate_half(values, position):
    full_width = values.shape[-1]
    half_width = full_width // 2
    frequency = ROPE_BASE ** (-jnp.arange(0, full_width, 2, dtype=jnp.float32) / full_width)
    angles = position.astype(jnp.float32)[:, None] * frequency[None, :]
    cosine = jnp.cos(angles)[:, None, :]
    sine_part = jnp.sin(angles)[:, None, :]
    first_half = values[..., :half_width]
    second_half = values[..., half_width:]
    return jnp.concatenate(
        [
            first_half * cosine - second_half * sine_part,
            first_half * sine_part + second_half * cosine,
        ],
        axis=-1,
    )


def grid_rotary(values, positions):
    half_width = values.shape[-1] // 2
    grid_row = positions // GRID_W
    column = positions % GRID_W
    return jnp.concatenate(
        [
            rotate_half(values[..., :half_width], grid_row),
            rotate_half(values[..., half_width:], column),
        ],
        axis=-1,
    )


def exchange_pieces(block_for, place, count, stride, axis_size):
    received = [block_for(place)]
    for hop in range(1, count):
        block = block_for((place + hop) % count)
        received.append(lax.ppermute(block, "sp", shifted(hop, count, stride, axis_size)))
    return received


def in_place_order(received, place):
    count = len(received)
    doubled = (received[::-1] * 2)[: 2 * count - 1]
    size = received[0].shape[0]
    whole = jnp.concatenate(doubled, axis=0)
    return lax.dynamic_slice_in_dim(whole, (count - 1 - place) * size, count * size, 0)


def shifted(hop, count, stride, axis_size):
    pairs = []
    for source in range(axis_size):
        group, rest = source // stride, source % stride
        pairs.append((source, ((group + hop) % count) * stride + rest))
    return pairs


def spread(block, count, stride):
    pieces = [block]
    for flip in range(1, stride):
        pairs = [
            (group * stride + rest, group * stride + (rest ^ flip))
            for group in range(count)
            for rest in range(stride)
        ]
        pieces.append(lax.ppermute(block, "sp", pairs))
    return pieces


def unflip(pieces, rest):
    bit = 1
    while bit < len(pieces):
        chosen = (rest & bit) != 0
        pieces = [
            jnp.where(chosen, pieces[at ^ bit], pieces[at]) for at in range(len(pieces))
        ]
        bit *= 2
    return pieces


def swap_cores(block):
    return lax.ppermute(block, "tp", [(0, 1), (1, 0)])


def attention_kernel(q_ref, k_ref, vt_ref, out_ref, *, span):
    queries = q_ref[...]
    rows, width = queries.shape
    run_max = jnp.full((1, rows), -1e30, jnp.float32)
    run_sum = jnp.zeros((1, rows), jnp.float32)
    run_acc = jnp.zeros((width, rows), jnp.float32)
    for start in range(0, k_ref.shape[0], span):
        scores = lax.dot_general(
            k_ref[start : start + span, :],
            queries,
            (((1,), (1,)), ((), ())),
            preferred_element_type=jnp.float32,
        )
        new_max = jnp.maximum(run_max, jnp.max(scores, axis=0, keepdims=True))
        probs = jnp.exp(scores - new_max)
        shrink = jnp.exp(run_max - new_max)
        run_sum = run_sum * shrink + jnp.sum(probs, axis=0, keepdims=True)
        run_acc = run_acc * shrink + jnp.dot(
            vt_ref[:, start : start + span],
            probs.astype(jnp.bfloat16),
            preferred_element_type=jnp.float32,
        )
        run_max = new_max
    out_ref[...] = (run_acc / run_sum).T.astype(jnp.bfloat16)


def attend(queries, keys, values_t):
    total, width = queries.shape
    key_count = keys.shape[0]
    block = math.gcd(total, 256)
    return pl.pallas_call(
        functools.partial(attention_kernel, span=math.gcd(key_count, 1024)),
        grid=(total // block,),
        out_shape=jax.ShapeDtypeStruct((total, width), jnp.bfloat16),
        in_specs=[
            pl.BlockSpec((block, width), lambda i: (i, 0)),
            pl.BlockSpec((key_count, width), lambda i: (0, 0)),
            pl.BlockSpec((width, key_count), lambda i: (0, 0)),
        ],
        out_specs=pl.BlockSpec((block, width), lambda i: (i, 0)),
        cost_estimate=pl.CostEstimate(
            flops=16 * total * key_count * width,
            bytes_accessed=4 * (total + key_count) * width,
            transcendentals=total * key_count,
        ),
    )(queries, keys, values_t)


def shards(
    query_proj,
    key_proj,
    value_proj,
    q_gain,
    k_gain,
    residual,
    out_weight,
    norm_gain,
    value_weight,
    gate_weight,
    down_weight,
    conv_value,
    conv_gate,
):
    tokens = query_proj.shape[0]
    heads_here = query_proj.shape[1] // HEAD_DIM
    kv_here = key_proj.shape[1] // HEAD_DIM
    group_size = heads_here // kv_here
    sp_size, tp_size = lax.axis_size("sp"), lax.axis_size("tp")
    count = math.gcd(sp_size, 4)
    stride = sp_size // count
    me, core = lax.axis_index("sp"), lax.axis_index("tp")
    place, rest = me // stride, me % stride
    positions = me * tokens + jnp.arange(tokens, dtype=jnp.int32)

    queries = grid_rotary(
        rms_norm(query_proj.reshape(tokens, heads_here, HEAD_DIM), q_gain), positions
    ) * HEAD_DIM ** (-0.5)
    queries = queries.astype(jnp.bfloat16)
    keys_rot = grid_rotary(
        rms_norm(key_proj.reshape(tokens, kv_here, HEAD_DIM), k_gain), positions
    ).astype(jnp.bfloat16)
    values = value_proj.reshape(tokens, kv_here, HEAD_DIM)

    ff_here = value_weight.shape[1]
    depth_here = value_weight.shape[0]
    hidden_here = ff_here // count

    split_heads = count if kv_here % count == 0 else 1
    kv_each = kv_here // split_heads
    packed = jnp.concatenate(
        [queries.reshape(tokens, kv_here, group_size * HEAD_DIM), keys_rot, values], axis=2
    ).transpose(1, 0, 2)
    packed = packed.reshape(split_heads, kv_each, tokens, (group_size + 2) * HEAD_DIM)
    if split_heads > 1:
        got = exchange_pieces(
            lambda at: lax.dynamic_index_in_dim(packed, at, 0, keepdims=False),
            place,
            count,
            stride,
            sp_size,
        )
        got, weights_in = lax.optimization_barrier((got, (value_weight, gate_weight, down_weight)))
    else:
        got, weights_in = [packed[0]], (value_weight, gate_weight, down_weight)
    value_in, gate_in, down_in = weights_in

    q_width = group_size * HEAD_DIM
    kv_mine = jnp.stack([piece[..., q_width:] for piece in got])
    if split_heads > 1:
        kv_all = jnp.stack(spread(kv_mine, count, stride))
    else:
        kv_all = lax.all_gather(kv_mine, "sp", axis=0)
    kv_all = kv_all.transpose(2 + 0, 0, 1, 3, 4).reshape(kv_each, sp_size * tokens, 2 * HEAD_DIM)

    def up_block(at):
        start = at * hidden_here
        return jnp.concatenate(
            [
                lax.dynamic_slice_in_dim(value_in, start, hidden_here, 1),
                lax.dynamic_slice_in_dim(gate_in, start, hidden_here, 1),
            ],
            axis=1,
        )

    def down_block(at):
        return lax.dynamic_slice_in_dim(down_in, at * hidden_here, hidden_here, 0)

    up_got = exchange_pieces(up_block, place, count, stride, sp_size)
    up_pieces = spread(in_place_order(up_got, place), count, stride)
    columns_here = down_weight.shape[1]
    down_got = exchange_pieces(down_block, place, count, stride, sp_size)
    down_cols = in_place_order(down_got, place).reshape(count, hidden_here, columns_here)
    down_cols = jnp.concatenate([down_cols[at] for at in range(count)], axis=1)
    down_pieces = spread(down_cols, count, stride)

    q_pieces = [piece[..., :q_width] for piece in got]
    per_head = []
    for kv_at in range(kv_each):
        keys_h = kv_all[kv_at, :, :HEAD_DIM]
        values_t = kv_all[kv_at, :, HEAD_DIM:].T
        per_group = []
        for group_at in range(group_size):
            columns = slice(group_at * HEAD_DIM, (group_at + 1) * HEAD_DIM)
            q_here = jnp.concatenate([piece[kv_at, :, columns] for piece in q_pieces], axis=0)
            per_group.append(attend(q_here, keys_h, values_t))
        per_head.append(jnp.concatenate(per_group, axis=1))
    done = jnp.concatenate(per_head, axis=1).reshape(len(got), tokens, -1)
    if split_heads > 1:
        back = [done[0]]
        for hop in range(1, count):
            back.append(lax.ppermute(done[hop], "sp", shifted(-hop, count, stride, sp_size)))
        attended = jnp.roll(jnp.stack(back), place, axis=0).transpose(1, 0, 2)
        attended = attended.reshape(tokens, heads_here * HEAD_DIM)
    else:
        attended = done[0]

    row_share = tokens // tp_size
    residual_mine = lax.dynamic_slice_in_dim(residual, core * row_share, row_share, 0)
    if tp_size == 2:
        weight_other = swap_cores(out_weight)
        halves = attended.reshape(2, row_share, heads_here * HEAD_DIM)
        rows_mine = lax.dynamic_index_in_dim(halves, core, 0, keepdims=False)
        rows_other = swap_cores(lax.dynamic_index_in_dim(halves, 1 - core, 0, keepdims=False))
        mix_mine = jnp.dot(rows_mine, out_weight, preferred_element_type=jnp.float32)
        mix_other = jnp.dot(rows_other, weight_other, preferred_element_type=jnp.float32)
        mix_out = (
            mix_mine.astype(jnp.bfloat16).astype(jnp.float32)
            + mix_other.astype(jnp.bfloat16).astype(jnp.float32)
        ).astype(jnp.bfloat16)
    else:
        mix_out = lax.psum_scatter(
            jnp.dot(attended, out_weight, preferred_element_type=jnp.float32).astype(jnp.bfloat16),
            "tp",
            scatter_dimension=0,
            tiled=True,
        )
    updated = (residual_mine.astype(jnp.float32) + mix_out.astype(jnp.float32)).astype(jnp.bfloat16)
    normed = rms_norm(updated, norm_gain).astype(jnp.bfloat16)
    width = normed.shape[1]
    normed = jnp.stack(
        [
            jnp.concatenate(
                [
                    normed[:, (at * stride + flip) * depth_here :][:, :depth_here]
                    for at in range(count)
                ],
                axis=1,
            )
            for flip in range(stride)
        ]
    )

    ups = []
    for hop in range(count):
        rows = normed
        if hop:
            rows = lax.ppermute(normed, "sp", shifted(hop, count, stride, sp_size))
        if tp_size == 2:
            other = swap_cores(rows)
            rows = jnp.concatenate(
                [jnp.where(core == 0, rows, other), jnp.where(core == 0, other, rows)], axis=1
            )
        else:
            rows = lax.all_gather(rows, "tp", axis=1, tiled=True)
        total = 0.0
        for flip in range(stride):
            part = lax.dynamic_index_in_dim(rows, rest ^ flip, 0, keepdims=False)
            total = total + jnp.dot(part, up_pieces[flip], preferred_element_type=jnp.float32)
        ups.append(total.astype(jnp.bfloat16))
    ups = jnp.stack(ups)

    forward = [
        (group * stride + at, group * stride + (at + 1) % stride)
        for group in range(count)
        for at in range(stride)
    ]
    backward = [(target, source) for source, target in forward]
    before = lax.ppermute(ups[:, -1], "sp", forward)
    after = lax.ppermute(ups[:, 0], "sp", backward)
    hops = jnp.arange(count)
    block_at = (place - hops) % count
    no_before = (rest == 0) & (block_at == 0)
    no_after = (rest == stride - 1) & (block_at == count - 1)
    before = jnp.where(rest == 0, jnp.roll(before, -1, axis=0), before)
    after = jnp.where(rest == stride - 1, jnp.roll(after, 1, axis=0), after)
    before = jnp.where(no_before[:, None], 0, before)
    after = jnp.where(no_after[:, None], 0, after)
    padded = jnp.concatenate([before[:, None], ups, after[:, None]], axis=1).astype(jnp.float32)
    taps = jnp.concatenate(
        [
            lax.dynamic_slice_in_dim(conv_value, place * hidden_here, hidden_here, 1),
            lax.dynamic_slice_in_dim(conv_gate, place * hidden_here, hidden_here, 1),
        ],
        axis=1,
    )
    conv = padded[:, :-2] * taps[0] + padded[:, 1:-1] * taps[1] + padded[:, 2:] * taps[2]
    hidden = (
        jax.nn.gelu(conv[..., hidden_here:], approximate=True) * conv[..., :hidden_here]
    ).astype(jnp.bfloat16)

    down_all = jnp.concatenate(down_pieces, axis=1)
    branch = 0.0
    for hop in list(range(1, count)) + [0]:
        partial = jnp.dot(hidden[hop], down_all, preferred_element_type=jnp.float32)
        if tp_size == 2:
            partial = partial.reshape(2, row_share, width)
            mine = lax.dynamic_index_in_dim(partial, core, 0, keepdims=False)
            theirs = lax.dynamic_index_in_dim(partial, 1 - core, 0, keepdims=False)
            other = swap_cores(theirs.astype(jnp.bfloat16))
            mine = mine + other.astype(jnp.float32)
        else:
            mine = lax.psum_scatter(
                partial.astype(jnp.bfloat16), "tp", scatter_dimension=0, tiled=True
            )
        if hop:
            mine = lax.ppermute(
                mine.astype(jnp.bfloat16), "sp", shifted(-hop, count, stride, sp_size)
            )
        branch = branch + mine.astype(jnp.float32)
    branch = branch.astype(jnp.bfloat16)
    span = count * columns_here
    pieces = unflip([branch[:, at * span : (at + 1) * span] for at in range(stride)], rest)
    branch = jnp.concatenate(
        [
            pieces[at][:, group * columns_here : (group + 1) * columns_here]
            for group in range(count)
            for at in range(stride)
        ],
        axis=1,
    )
    return (updated.astype(jnp.float32) + branch.astype(jnp.float32)).astype(jnp.bfloat16)


def fused_kernel(
    query, key, value, q_gain, k_gain, cosine, sine, res_in, wo_in, gain, wv_in, wg_in, wd_in, taps_v, taps_g, out,
    q_in, kv_in, qraw, qhead, kvbuf, kbuf, vbuf, top, total, acc, att_send, att_all, wo, res, mix_send, mix_recv,
    own_mix, upd, rows, wup, wdown, ups, hidden, part_keep, part_send, part_recv, red_send,
    red_recv, fin, local_sem, send_sem, recv_sem,
):
    sp, core = lax.axis_index("sp"), lax.axis_index("tp")
    x, y, zl, zh = sp % 2, (sp // 2) % 2, (sp // 4) % 2, sp // 8
    fx, fy, fl, fh = 1 - 2 * x, 1 - 2 * y, 1 - 2 * zl, 1 - 2 * zh
    depth = wv_in.shape[0]
    ffs = wdown.shape[1]
    pairs, half, pair_w = upd.shape
    tokens = 2 * half
    other = 1 - core

    def xs(flip):
        return x + fx * flip

    def mate(at):
        return sp + fx * (at % 2) + 4 * fl * (at // 2)

    def place(at):
        return xs(at % 2) + 2 * (zl + fl * (at // 2))

    mine = place(0)
    y_mate, z_mate = sp + 2 * fy, sp + 8 * fh
    diag_mate = sp + 2 * fy + 8 * fh

    def pair_at(rel):
        return (y + fy * (rel % 2)) + 2 * (zl + fl * ((rel // 2) % 2)) + 4 * (zh + fh * (rel // 4))

    ids = {}
    started = []

    def remote(name, src, dst, device):
        at = ids.setdefault(name, len(ids))
        assert at < send_sem.shape[0], len(ids)
        return pltpu.make_async_remote_copy(
            src_ref=src, dst_ref=dst, send_sem=send_sem.at[at], recv_sem=recv_sem.at[at],
            device_id=device, device_id_type=pl.DeviceIdType.MESH,
        )

    def send(name, src, dst, device):
        copy = remote(name, src, dst, device)
        copy.start()
        started.append(copy)

    def arrived(name, dst):
        remote(name, dst, dst, (sp, core)).wait_recv()

    def lanes(start, size):
        return pl.ds(pl.multiple_of(start, 128), size)

    barrier = pltpu.get_barrier_semaphore()
    partners = [(sp, other)] + [(mate(at), core) for at in (1, 2, 3)]
    partners += [(y_mate, core), (z_mate, core), (diag_mate, core)]
    for device in partners:
        pl.semaphore_signal(barrier, inc=1, device_id=device, device_id_type=pl.DeviceIdType.MESH)

    lane = lax.broadcasted_iota(jnp.int32, (tokens, 2 * HEAD_DIM), 1)
    left_head = lane < HEAD_DIM
    quarter = HEAD_DIM // 4
    low = lane % (2 * quarter) < quarter
    lanes_all = 2 * HEAD_DIM
    q_row, k_row = (jnp.concatenate([ref[...], ref[...]], axis=1) for ref in (q_gain, k_gain))

    def rotate(heads_pair, gain_row, scale):
        wide = heads_pair.astype(jnp.float32)
        squares = wide * wide
        left = jnp.sum(jnp.where(left_head, squares, 0.0), axis=1, keepdims=True)
        right = jnp.sum(jnp.where(left_head, 0.0, squares), axis=1, keepdims=True)
        mean = jnp.where(left_head, left, right) / HEAD_DIM
        normed = wide * lax.rsqrt(mean + NORM_EPS) * gain_row
        swapped = jnp.where(
            low,
            pltpu.roll(normed, lanes_all - quarter, 1),
            pltpu.roll(normed, quarter, 1),
        )
        return (normed * cosine[...] + swapped * sine[...]) * scale

    for m in range(key.shape[1] // lanes_all):
        cols = slice(m * lanes_all, (m + 1) * lanes_all)
        turned = rotate(key[:, cols], k_row, 1.0)
        passed = value[:, cols].astype(jnp.float32)
        first = jnp.where(left_head, turned, pltpu.roll(passed, HEAD_DIM, 1))
        second = jnp.where(left_head, pltpu.roll(turned, HEAD_DIM, 1), passed)
        kv_in[2 * m] = first.astype(jnp.bfloat16)
        kv_in[2 * m + 1] = second.astype(jnp.bfloat16)
    pl.semaphore_wait(barrier, len(partners))

    def piece(kind, rel, x_at):
        start = pl.multiple_of(x_at * depth, depth)
        if kind == "v":
            return wup.at[rel, pl.ds(start, depth), pl.ds(0, ffs)]
        if kind == "g":
            return wup.at[rel, pl.ds(start, depth), pl.ds(ffs, ffs)]
        return wdown.at[rel, :, pl.ds(start, depth)]

    def whole(kind, rel):
        if kind == "v":
            return wup.at[rel, :, pl.ds(0, ffs)]
        if kind == "g":
            return wup.at[rel, :, pl.ds(ffs, ffs)]
        return wdown.at[rel]

    def shard(kind, at):
        if kind == "d":
            return wd_in.at[pl.ds(pl.multiple_of(place(at) * ffs, 128), ffs), :]
        return (wv_in if kind == "v" else wg_in).at[:, lanes(place(at) * ffs, ffs)]

    def launch(name, src, dst, device, where):
        fresh = name not in ids
        copy = remote(name, src, dst, device)
        if where is None:
            copy.start()
        else:
            pl.when(where)(copy.start)
        if fresh:
            started.append(copy)

    def exchange(kind, at, where=None):
        dst = piece(kind, 2 * (at // 2), x)
        launch(f"w1{kind}{at}", shard(kind, at), dst, (mate(at), core), where)

    def exchanged(kind, at):
        arrived(f"w1{kind}{at}", piece(kind, 2 * (at // 2), xs(at % 2)))

    inner, outer = zl != zh, zl == zh

    def across(kind, at, where=None):
        src = piece(kind, 2 * (at // 2), xs(at % 2)) if at else shard(kind, 0)
        dst = piece(kind, 2 * (at // 2) + 4, xs(at % 2))
        launch(f"wz{kind}{at}", src, dst, (z_mate, core), where)

    def crossed(kind, at):
        arrived(f"wz{kind}{at}", piece(kind, 2 * (at // 2) + 4, xs(at % 2)))

    def sideways(kind, rel, where=None):
        launch(f"wy{kind}{rel}", whole(kind, rel), whole(kind, rel + 1), (y_mate, core), where)

    def sideways_half(kind, at):
        src = piece(kind, 0, xs(at)) if at else shard(kind, 0)
        send(f"wy{kind}h{at}", src, piece(kind, 1, xs(at)), (y_mate, core))

    def from_side(kind, rel):
        if rel or kind == "d":
            arrived(f"wy{kind}{rel}", whole(kind, rel + 1))
        else:
            arrived(f"wy{kind}h0", piece(kind, 1, x))
            arrived(f"wy{kind}h1", piece(kind, 1, xs(1)))

    for at in (2, 3, 1):
        send(f"kv{at}", kv_in.at[place(at)], kvbuf.at[0, mine], (mate(at), core))
    for m in range(q_in.shape[0]):
        cols = slice(m * lanes_all, (m + 1) * lanes_all)
        q_in[m] = rotate(query[:, cols], q_row, HEAD_DIM ** (-0.5)).astype(jnp.bfloat16)
    for at in (2, 3, 1):
        send(f"q{at}", q_in.at[place(at)], qraw.at[mine], (mate(at), core))
    locals_ = [
        pltpu.make_async_copy(shard(kind, 0), piece(kind, 0, x), local_sem.at[n])
        for n, kind in enumerate("vgd")
    ]
    locals_.append(pltpu.make_async_copy(wo_in, wo, local_sem.at[3]))
    locals_.append(
        pltpu.make_async_copy(
            res_in.at[pl.ds(pl.multiple_of(core * half, half), half), :], res, local_sem.at[4]
        )
    )
    for copy in locals_:
        copy.start()
    qraw[mine] = q_in[mine]
    kvbuf[0, mine] = kv_in[mine]
    top[...] = jnp.full(top.shape, -1e30, jnp.float32)
    total[...] = jnp.zeros(total.shape, jnp.float32)
    acc[...] = jnp.zeros(acc.shape, jnp.float32)
    for at in (1, 2, 3):
        arrived(f"kv{at}", kvbuf.at[0, place(at)])
    send("kvz", kvbuf.at[0], kvbuf.at[2], (z_mate, core))
    send("kvy", kvbuf.at[0], kvbuf.at[1], (y_mate, core))
    sideways_half("v", 0)
    for at in (1, 2, 3):
        arrived(f"q{at}", qraw.at[place(at)])
    across("v", 0)
    for at in (1, 2, 3):
        exchange("v", at)
    sideways_half("g", 0)
    for at in (2, 3, 1):
        exchange("g", at)
    width = HEAD_DIM
    group = qraw.shape[2] // width
    blocks = qraw.shape[0]

    @pl.loop(0, blocks)
    def _(b):
        for a in range(group):
            qhead[b * group + a] = qraw[b][:, a * width : (a + 1) * width]

    def unpack(t):
        @pl.loop(0, blocks)
        def _(b):
            start = pl.multiple_of(b * tokens, tokens)
            pair = kvbuf[t, b]
            kbuf[t, pl.ds(start, tokens), :] = pair[:, :width]
            vbuf[t, :, pl.ds(start, tokens)] = pair[:, width:].T

    def attend_block(t, h):
        scores = lax.dot_general(
            kbuf[t], qhead[h], (((1,), (1,)), ((), ())), preferred_element_type=jnp.float32
        )
        old = top[h]
        new = jnp.maximum(old, jnp.max(scores, axis=0, keepdims=True))
        probs = jnp.exp(scores - new)
        shrink = jnp.exp(old - new)
        total[h] = total[h] * shrink + jnp.sum(probs, axis=0, keepdims=True)
        acc[h] = acc[h] * shrink + jnp.dot(
            vbuf[t], probs.astype(jnp.bfloat16), preferred_element_type=jnp.float32
        )
        top[h] = new

    def attend_some(t, lo, hi):
        @pl.loop(lo, hi)
        def _(h):
            attend_block(t, h)

    heads = blocks * group
    unpack(0)
    attend_some(0, 0, heads // 2)
    for copy in locals_[:3]:
        copy.wait()
    exchanged("v", 1)
    across("v", 1)
    sideways_half("v", 1)
    across("g", 0)
    attend_some(0, heads // 2, heads)
    arrived("kvy", kvbuf.at[1])
    unpack(1)
    attend_some(1, 0, heads // 2)
    exchanged("g", 1)
    across("g", 1)
    sideways_half("g", 1)
    attend_some(1, heads // 2, heads)
    arrived("kvz", kvbuf.at[2])
    send("kvd", kvbuf.at[2], kvbuf.at[3], (y_mate, core))
    unpack(2)
    attend_some(2, 0, heads // 2)
    exchanged("v", 2)
    exchanged("v", 3)
    sideways("v", 2)
    across("v", 2)
    across("v", 3)
    attend_some(2, heads // 2, heads)
    arrived("kvd", kvbuf.at[3])
    unpack(3)

    def finish(block):
        first = block * group
        pieces = [acc[first + a] / total[first + a] for a in range(group)]
        return jnp.concatenate(pieces, axis=0).T.astype(jnp.bfloat16)

    for at in (2, 3, 1, 0):
        block = place(at)
        attend_some(3, block * group, block * group + group)
        if at:
            att_send[at - 1] = finish(block)
            send(f"att{at}", att_send.at[at - 1], att_all.at[mine], (mate(at), core))
        else:
            att_all[mine] = finish(block)
    exchanged("g", 2)
    exchanged("g", 3)
    sideways("g", 2)
    exchange("d", 1)
    for copy in locals_[3:]:
        copy.wait()
    for at in (1, 2, 3):
        arrived(f"att{at}", att_all.at[place(at)])
    crossed("v", 0)
    crossed("v", 1)
    sideways("v", 4)

    def project(n, rows_at):
        start = pl.multiple_of(rows_at * half, half)
        left = jnp.concatenate([att_all[b, pl.ds(start, half), :] for b in range(blocks)], axis=1)
        return jnp.dot(left, wo[:, lanes(n * pair_w, pair_w)], preferred_element_type=jnp.float32)

    @pl.loop(0, pairs)
    def _(n):
        mix_send[n] = project(n, other).astype(jnp.bfloat16)

    send("mix", mix_send, mix_recv, (sp, other))

    @pl.loop(0, pairs)
    def _(n):
        own_mix[n] = project(n, core).astype(jnp.bfloat16)

    arrived("mix", mix_recv)

    def update(n, squares):
        mixed = own_mix[n].astype(jnp.float32) + mix_recv[n].astype(jnp.float32)
        mixed = mixed.astype(jnp.bfloat16).astype(jnp.float32)
        held = res[:, lanes(n * pair_w, pair_w)].astype(jnp.float32)
        new = (held + mixed).astype(jnp.bfloat16)
        upd[n] = new
        wide = new.astype(jnp.float32)
        return squares + jnp.sum(wide * wide, axis=1, keepdims=True)

    squares = lax.fori_loop(0, pairs, update, jnp.zeros((half, 1), jnp.float32))
    inv = lax.rsqrt(squares / (pairs * pair_w) + NORM_EPS)
    my_rows = pl.ds(pl.multiple_of(core * half, half), half)

    @pl.loop(0, pairs)
    def _(n):
        scaled = upd[n].astype(jnp.float32) * inv * gain[:, lanes(n * pair_w, pair_w)]
        rows[mine, n, my_rows, :] = scaled.astype(jnp.bfloat16)

    def rows_of(g, at, part=None):
        cut = slice(None) if part is None else pl.ds(part * (pairs // 2), pairs // 2)
        return rows.at[g, cut, pl.ds(pl.multiple_of(at * half, half), half), :]

    def spread_rows(name, at_block, device, part=None):
        ref = rows_of(place(at_block), core, part)
        send(name, ref, ref, device)

    for part in (0, 1):
        spread_rows(f"row2{part}", 0, (mate(2), core), part)
        spread_rows(f"row1{1 - part}", 0, (mate(1), core), 1 - part)
    spread_rows("row0", 0, (sp, other))
    across("g", 2, outer)
    across("g", 3, outer)

    def up_dot(g, rels):
        left = jnp.concatenate([rows[g, pair_at(rel)] for rel in rels], axis=1)
        return left

    def up_block(g, rels, fresh):
        up_inner(g, rels, fresh)

    def up_inner(g, rels, fresh):
        seg, x_at = g // 2, g % 2
        start = pl.multiple_of(8 + x_at * tokens, 8)
        left = up_dot(g, rels)

        @pl.loop(0, 2 * ffs // pair_w)
        def _(n):
            cols = lanes(n * pair_w, pair_w)
            part = jnp.zeros((tokens, pair_w), jnp.float32)
            for i, rel in enumerate(rels):
                part = part + jnp.dot(
                    left[:, i * pair_w : (i + 1) * pair_w], wup[rel, :, cols],
                    preferred_element_type=jnp.float32,
                )
            if fresh:
                ups[seg, pl.ds(start, tokens), cols] = part
            else:
                ups[seg, pl.ds(start, tokens), cols] += part

    for kind in "vg":
        from_side(kind, 0)
        from_side(kind, 2)
    arrived("row0", rows_of(mine, other))
    up_block(mine, (0, 2, 1, 3), True)
    crossed("g", 0)
    crossed("g", 1)
    sideways("g", 4)
    arrived("row20", rows_of(place(2), core, 0))
    spread_rows("row30", 2, (mate(1), core), 0)
    arrived("row11", rows_of(place(1), core, 1))
    spread_rows("row31", 1, (mate(2), core), 1)
    exchanged("d", 1)
    across("d", 0, outer)
    across("d", 1, outer)
    for at in (2, 3):
        exchange("d", at, outer)
    arrived("row21", rows_of(place(2), core, 1))
    spread_rows("fwd2", 2, (sp, other))
    arrived("row10", rows_of(place(1), core, 0))
    spread_rows("fwd1", 1, (sp, other))
    sideways("d", 0)
    arrived("fwd2", rows_of(place(2), other))
    up_block(place(2), (0, 2, 1, 3), True)
    crossed("v", 2)
    crossed("v", 3)
    sideways("v", 6)
    across("g", 2, inner)
    across("g", 3, inner)
    for at in (2, 3):
        exchange("d", at, inner)
    arrived("fwd1", rows_of(place(1), other))
    up_block(place(1), (0, 2, 1, 3), True)
    arrived("row30", rows_of(place(3), core, 0))
    arrived("row31", rows_of(place(3), core, 1))
    spread_rows("fwd3", 3, (sp, other))
    across("d", 0, inner)
    across("d", 1, inner)
    arrived("fwd3", rows_of(place(3), other))
    up_block(place(3), (0, 2, 1, 3), True)
    crossed("g", 2)
    crossed("g", 3)
    sideways("g", 6)

    @pl.loop(0, blocks)
    def _(g):
        up_block(g, (4, 6), False)

    @pl.when(inner)
    def _():
        exchanged("d", 2)
        exchanged("d", 3)

    across("d", 2, inner)
    across("d", 3, inner)
    sideways("d", 2, inner)
    for kind in "vg":
        from_side(kind, 4)
        from_side(kind, 6)


    @pl.loop(0, blocks)
    def _(g):
        up_block(g, (5, 7), False)

    span = 2 * tokens
    head, tail = pl.ds(8, 8), pl.ds(span, 8)
    before, after = pl.ds(0, 8), pl.ds(span + 8, 8)
    even = y == 0

    def edge(name, seg_from, rows_from, seg_to, rows_to, device):
        send_at = remote(name, ups.at[seg_from, rows_from, :], ups.at[seg_to, rows_to, :], device)
        return send_at

    @pl.when(even)
    def _():
        edge("h0", 1, head, 0, after, (y_mate, core)).start()
        edge("h1", 0, tail, 0, before, (y_mate, core)).start()
        edge("h2", 1, tail, 1, before, (y_mate, core)).start()

        @pl.when(zh == 1)
        def _():
            edge("h3", 0, head, 1, after, (diag_mate, core)).start()

        @pl.when(zh == 0)
        def _():
            ups[0, before, :] = jnp.zeros((8, 2 * ffs), jnp.float32)

    @pl.when(y == 1)
    def _():
        edge("h0", 0, head, 0, after, (y_mate, core)).start()
        edge("h1", 1, head, 1, after, (y_mate, core)).start()
        edge("h2", 0, tail, 1, before, (y_mate, core)).start()

        @pl.when(zh == 0)
        def _():
            edge("h3", 1, tail, 0, before, (diag_mate, core)).start()

        @pl.when(zh == 1)
        def _():
            ups[1, after, :] = jnp.zeros((8, 2 * ffs), jnp.float32)

    tap_cols = lanes(mine * ffs, ffs)
    tv, tg = taps_v[:, tap_cols], taps_g[:, tap_cols]
    step = 64

    def convolve(window, taps):
        rounded = window.astype(jnp.bfloat16).astype(jnp.float32)
        return (
            rounded[7 : 7 + step] * taps[0:1]
            + rounded[8 : 8 + step] * taps[1:2]
            + rounded[9 : 9 + step] * taps[2:3]
        )

    def hidden_block(i):
        seg, at = i // (span // step), i % (span // step)
        window = pl.ds(pl.multiple_of(at * step, 8), step + 16)
        for n in range(ffs // 128):
            left, right = slice(n * 128, n * 128 + 128), slice(ffs + n * 128, ffs + n * 128 + 128)
            conv_v = convolve(ups[seg, window, left], tv[:, left])
            conv_g = convolve(ups[seg, window, right], tg[:, left])
            value = jax.nn.gelu(conv_g, approximate=True) * conv_v
            block, at_row = i // (tokens // step), (i % (tokens // step)) * step
            to = (at_row // half) * blocks * half + block * half + at_row % half
            hidden[pl.ds(pl.multiple_of(to, step), step), left] = value.astype(jnp.bfloat16)

    per = span // step

    @pl.loop(0, 2 * (per - 2))
    def _(i):
        seg = i // (per - 2)
        hidden_block(seg * per + 1 + i % (per - 2))

    @pl.when(even)
    def _():
        edge("h0", 0, head, 0, after, (sp, core)).wait_recv()
        edge("h1", 1, head, 1, after, (sp, core)).wait_recv()
        edge("h2", 0, tail, 1, before, (sp, core)).wait_recv()

        @pl.when(zh == 1)
        def _():
            edge("h3", 1, tail, 0, before, (sp, core)).wait_recv()

    @pl.when(y == 1)
    def _():
        edge("h0", 1, head, 0, after, (sp, core)).wait_recv()
        edge("h1", 0, tail, 0, before, (sp, core)).wait_recv()
        edge("h2", 1, tail, 1, before, (sp, core)).wait_recv()

        @pl.when(zh == 0)
        def _():
            edge("h3", 0, head, 1, after, (sp, core)).wait_recv()

    @pl.when(outer)
    def _():
        exchanged("d", 2)
        exchanged("d", 3)

    across("d", 2, outer)
    across("d", 3, outer)
    sideways("d", 2, outer)
    crossed("d", 0)
    crossed("d", 1)
    sideways("d", 4)

    @pl.loop(0, 4)
    def _(i):
        hidden_block((i // 2) * per + (i % 2) * (per - 1))

    order = [0, 2, 1, 3, 4, 6, 5, 7]
    straight = order[-4:]

    def down(rel):
        def product(at):
            left = hidden[pl.ds(pl.multiple_of(at * blocks * half, half), blocks * half), :]
            whole_part = jnp.dot(left, wdown[rel], preferred_element_type=jnp.float32)
            return whole_part.reshape(blocks, half, pair_w)

        part_send[rel] = product(other).astype(jnp.bfloat16)
        send(f"part{rel}", part_send.at[rel], part_recv.at[rel], (sp, other))
        part_keep[order.index(rel) % 2] = product(core)

    def merge(rel):
        arrived(f"part{rel}", part_recv.at[rel])

        def both(at):
            g = place(at)
            return part_keep[order.index(rel) % 2, g] + part_recv[rel, g].astype(jnp.float32)

        if rel in straight:
            for at in (2, 3, 1):
                red_send[rel, at - 1] = both(at).astype(jnp.bfloat16)
                to = across_rel(rel, at)
                send(f"red{to}{at}", red_send.at[rel, at - 1], red_recv.at[to, at - 1],
                     (mate(at), core))
            fin[rel, 0] = both(0)
            return
        first, second = ways()
        for i, at in enumerate((first, 3)):
            red_send[rel, i] = both(at).astype(jnp.bfloat16)
        to = across_rel(rel, first)
        send(f"reda{to}", red_send.at[rel, pl.ds(0, 2)], red_recv.at[to, pl.ds(0, 2)],
             (mate(first), core))
        fin[rel, 0] = both(0)
        fin[rel, 1] = both(second)

    def ways():
        return (1, 2)

    def across_rel(rel, at):
        return rel ^ (at & 2)

    def pass_on(rel):
        second = ways()[1]
        arrived(f"reda{rel}", red_recv.at[rel, pl.ds(0, 2)])
        red_send[rel, 2] = (fin[rel, 1] + red_recv[rel, 1].astype(jnp.float32)).astype(jnp.bfloat16)
        to = across_rel(rel, second)
        send(f"redb{to}", red_send.at[rel, 2], red_recv.at[to, 2], (mate(second), core))

    def close(rel):
        branch = fin[rel, 0]
        if rel in straight:
            for at in (1, 2, 3):
                arrived(f"red{rel}{at}", red_recv.at[rel, at - 1])
                branch = branch + red_recv[rel, at - 1].astype(jnp.float32)
        else:
            arrived(f"redb{rel}", red_recv.at[rel, 2])
            branch = branch + red_recv[rel, 0].astype(jnp.float32)
            branch = branch + red_recv[rel, 2].astype(jnp.float32)
        n = pair_at(rel)
        wide = branch.astype(jnp.bfloat16).astype(jnp.float32)
        new = (upd[n].astype(jnp.float32) + wide).astype(jnp.bfloat16)
        out[:, lanes(n * pair_w, pair_w)] = new

    down(0)
    for i, rel in enumerate(order[1:]):
        if rel == 1:
            from_side("d", 0)
        if rel == 3:
            from_side("d", 2)
        if rel == 4:
            crossed("d", 2)
            crossed("d", 3)
            sideways("d", 6)
        if rel == 5:
            from_side("d", 4)
        if rel == 7:
            from_side("d", 6)
        down(rel)
        merge(order[i])
        if i >= 2 and order[i - 2] not in straight:
            pass_on(order[i - 2])
    merge(order[-1])
    for rel in order:
        close(rel)
    for copy in started:
        copy.wait_send()
    for name in ("h0", "h1", "h2"):
        edge(name, 0, head, 0, after, (sp, core)).wait_send()

    @pl.when((y + zh) == 1)
    def _():
        edge("h3", 0, head, 0, after, (sp, core)).wait_send()


def fused(query_proj, key_proj, value_proj, gains, tables, residual, out_weight, norm_gain,
          value_weight, gate_weight, down_weight, conv_value, conv_gate):
    groups, tokens = key_proj.shape[1] // HEAD_DIM, query_proj.shape[0]
    q_width = query_proj.shape[1] // groups
    half, width = tokens // 2, residual.shape[1]
    depth, ff_here = value_weight.shape
    pair_w = 2 * depth
    pairs = width // pair_w
    ffs = ff_here // groups
    heads = groups * (q_width // HEAD_DIM)
    keys = groups * tokens
    bf16, f32 = jnp.bfloat16, jnp.float32
    vmem, anywhere = pl.BlockSpec(memory_space=pltpu.VMEM), pl.BlockSpec(memory_space=pl.ANY)
    copies = 104
    return pl.pallas_call(
        fused_kernel,
        out_shape=jax.ShapeDtypeStruct((half, width), bf16),
        in_specs=[vmem] * 7 + [anywhere, anywhere, vmem, anywhere, anywhere, anywhere, vmem, vmem],
        out_specs=vmem,
        scratch_shapes=[
            pltpu.VMEM((groups, tokens, q_width), bf16),
            pltpu.VMEM((groups, tokens, 2 * HEAD_DIM), bf16),
            pltpu.VMEM((groups, tokens, q_width), bf16),
            pltpu.VMEM((heads, tokens, HEAD_DIM), bf16),
            pltpu.VMEM((4, groups, tokens, 2 * HEAD_DIM), bf16),
            pltpu.VMEM((4, keys, HEAD_DIM), bf16),
            pltpu.VMEM((4, HEAD_DIM, keys), bf16),
            pltpu.VMEM((heads, 1, tokens), f32),
            pltpu.VMEM((heads, 1, tokens), f32),
            pltpu.VMEM((heads, HEAD_DIM, tokens), f32),
            pltpu.VMEM((groups - 1, tokens, q_width), bf16),
            pltpu.VMEM((groups, tokens, q_width), bf16),
            pltpu.VMEM(out_weight.shape, bf16),
            pltpu.VMEM((half, width), bf16),
            pltpu.VMEM((pairs, half, pair_w), bf16),
            pltpu.VMEM((pairs, half, pair_w), bf16),
            pltpu.VMEM((pairs, half, pair_w), bf16),
            pltpu.VMEM((pairs, half, pair_w), bf16),
            pltpu.VMEM((groups, pairs, tokens, pair_w), bf16),
            pltpu.VMEM((pairs, pair_w, 2 * ffs), bf16),
            pltpu.VMEM((pairs, ffs, pair_w), bf16),
            pltpu.VMEM((2, 2 * tokens + 16, 2 * ffs), f32),
            pltpu.VMEM((keys, ffs), bf16),
            pltpu.VMEM((2, groups, half, pair_w), f32),
            pltpu.VMEM((pairs, groups, half, pair_w), bf16),
            pltpu.VMEM((pairs, groups, half, pair_w), bf16),
            pltpu.VMEM((pairs, groups - 1, half, pair_w), bf16),
            pltpu.VMEM((pairs, groups - 1, half, pair_w), bf16),
            pltpu.VMEM((pairs, 2, half, pair_w), f32),
            pltpu.SemaphoreType.DMA((5,)),
            pltpu.SemaphoreType.DMA((copies,)),
            pltpu.SemaphoreType.DMA((copies,)),
        ],
        compiler_params=pltpu.CompilerParams(
            collective_id=0, has_side_effects=True, vmem_limit_bytes=60 * 2**20
        ),
    )(query_proj, key_proj, value_proj, *gains, *tables, residual, out_weight, norm_gain[None, :], value_weight, gate_weight,
      down_weight, conv_value, conv_gate)


def fused_layer(
    query_proj, key_proj, value_proj, q_gain, k_gain, residual, out_weight, norm_gain,
    value_weight, gate_weight, down_weight, conv_value, conv_gate,
):
    tokens, width = query_proj.shape[0], 2 * HEAD_DIM
    positions = lax.axis_index("sp") * tokens + lax.broadcasted_iota(jnp.int32, (tokens, width), 0)
    lane = lax.broadcasted_iota(jnp.int32, (tokens, width), 1)
    half = HEAD_DIM // 2
    frequency = ROPE_BASE ** (-np.arange(0, half, 2, dtype=np.float32) / half)
    frequency = np.tile(frequency.astype(np.float32), width // (half // 2))[None, :]
    in_first = lane % HEAD_DIM < half
    place = jnp.where(in_first, positions // GRID_W, positions % GRID_W)
    angle = place.astype(jnp.float32) * frequency
    sign = jnp.where(lane % half < half // 2, -1.0, 1.0)
    tables = (jnp.cos(angle), jnp.sin(angle) * sign)
    gains = (q_gain[None, :], k_gain[None, :])
    return fused(query_proj, key_proj, value_proj, gains, tables, residual, out_weight, norm_gain,
                 value_weight, gate_weight, down_weight, conv_value, conv_gate)


def fits(sp_size, tp_size, arrays):
    tokens, kv_here = arrays[0].shape[0], arrays[1].shape[1] // HEAD_DIM
    depth, ff_here = arrays[8].shape
    return (
        (sp_size, tp_size, kv_here) == (16, 2, 4)
        and depth % 128 == 0
        and arrays[0].shape[1] == 2 * arrays[1].shape[1]
        and ff_here % (kv_here * 128) == 0
        and (2 * ff_here // kv_here) % (2 * depth) == 0
        and tokens % 256 == 0
    )


def layer(*arrays):
    if fits(lax.axis_size("sp"), lax.axis_size("tp"), arrays):
        return fused_layer(*arrays)
    return shards(*arrays)


def solution(mesh):
    return jax.shard_map(
        layer,
        mesh=mesh,
        in_specs=(
            P("sp", "tp"),
            P("sp", "tp"),
            P("sp", "tp"),
            P(),
            P(),
            P("sp", None),
            P("tp", None),
            P(),
            P("sp", "tp"),
            P("sp", "tp"),
            P("tp", "sp"),
            P(None, "tp"),
            P(None, "tp"),
        ),
        out_specs=P(("sp", "tp"), None),
        check_vma=False,
    )
```

```python
import functools
import math

import jax
import jax.numpy as jnp
import numpy as np
from jax import lax
from jax.experimental import pallas as pl
from jax.experimental.pallas import tpu as pltpu
from jax.sharding import PartitionSpec as P


HEAD_DIM = 64
GRID_W = 64


NORM_EPS = 1e-06
ROPE_BASE = 10000.0


def rms_norm(block_in, gain_vec):
    values = block_in.astype(jnp.float32)
    inv_rms = lax.rsqrt(jnp.mean(values * values, axis=-1, keepdims=True) + NORM_EPS)
    return values * inv_rms * gain_vec


def rotate_half(values, position):
    full_width = values.shape[-1]
    half_width = full_width // 2
    frequency = ROPE_BASE ** (-jnp.arange(0, full_width, 2, dtype=jnp.float32) / full_width)
    angles = position.astype(jnp.float32)[:, None] * frequency[None, :]
    cosine = jnp.cos(angles)[:, None, :]
    sine_part = jnp.sin(angles)[:, None, :]
    first_half = values[..., :half_width]
    second_half = values[..., half_width:]
    return jnp.concatenate(
        [
            first_half * cosine - second_half * sine_part,
            first_half * sine_part + second_half * cosine,
        ],
        axis=-1,
    )


def grid_rotary(values, positions):
    half_width = values.shape[-1] // 2
    grid_row = positions // GRID_W
    column = positions % GRID_W
    return jnp.concatenate(
        [
            rotate_half(values[..., :half_width], grid_row),
            rotate_half(values[..., half_width:], column),
        ],
        axis=-1,
    )


def exchange_pieces(block_for, place, count, stride, axis_size):
    received = [block_for(place)]
    for hop in range(1, count):
        block = block_for((place + hop) % count)
        received.append(lax.ppermute(block, "sp", shifted(hop, count, stride, axis_size)))
    return received


def in_place_order(received, place):
    count = len(received)
    doubled = (received[::-1] * 2)[: 2 * count - 1]
    size = received[0].shape[0]
    whole = jnp.concatenate(doubled, axis=0)
    return lax.dynamic_slice_in_dim(whole, (count - 1 - place) * size, count * size, 0)


def shifted(hop, count, stride, axis_size):
    pairs = []
    for source in range(axis_size):
        group, rest = source // stride, source % stride
        pairs.append((source, ((group + hop) % count) * stride + rest))
    return pairs


def spread(block, count, stride):
    pieces = [block]
    for flip in range(1, stride):
        pairs = [
            (group * stride + rest, group * stride + (rest ^ flip))
            for group in range(count)
            for rest in range(stride)
        ]
        pieces.append(lax.ppermute(block, "sp", pairs))
    return pieces


def unflip(pieces, rest):
    bit = 1
    while bit < len(pieces):
        chosen = (rest & bit) != 0
        pieces = [
            jnp.where(chosen, pieces[at ^ bit], pieces[at]) for at in range(len(pieces))
        ]
        bit *= 2
    return pieces


def swap_cores(block):
    return lax.ppermute(block, "tp", [(0, 1), (1, 0)])


def attention_kernel(q_ref, k_ref, vt_ref, out_ref, *, span):
    queries = q_ref[...]
    rows, width = queries.shape
    run_max = jnp.full((1, rows), -1e30, jnp.float32)
    run_sum = jnp.zeros((1, rows), jnp.float32)
    run_acc = jnp.zeros((width, rows), jnp.float32)
    for start in range(0, k_ref.shape[0], span):
        scores = lax.dot_general(
            k_ref[start : start + span, :],
            queries,
            (((1,), (1,)), ((), ())),
            preferred_element_type=jnp.float32,
        )
        new_max = jnp.maximum(run_max, jnp.max(scores, axis=0, keepdims=True))
        probs = jnp.exp(scores - new_max)
        shrink = jnp.exp(run_max - new_max)
        run_sum = run_sum * shrink + jnp.sum(probs, axis=0, keepdims=True)
        run_acc = run_acc * shrink + jnp.dot(
            vt_ref[:, start : start + span],
            probs.astype(jnp.bfloat16),
            preferred_element_type=jnp.float32,
        )
        run_max = new_max
    out_ref[...] = (run_acc / run_sum).T.astype(jnp.bfloat16)


def attend(queries, keys, values_t):
    total, width = queries.shape
    key_count = keys.shape[0]
    block = math.gcd(total, 256)
    return pl.pallas_call(
        functools.partial(attention_kernel, span=math.gcd(key_count, 1024)),
        grid=(total // block,),
        out_shape=jax.ShapeDtypeStruct((total, width), jnp.bfloat16),
        in_specs=[
            pl.BlockSpec((block, width), lambda i: (i, 0)),
            pl.BlockSpec((key_count, width), lambda i: (0, 0)),
            pl.BlockSpec((width, key_count), lambda i: (0, 0)),
        ],
        out_specs=pl.BlockSpec((block, width), lambda i: (i, 0)),
        cost_estimate=pl.CostEstimate(
            flops=16 * total * key_count * width,
            bytes_accessed=4 * (total + key_count) * width,
            transcendentals=total * key_count,
        ),
    )(queries, keys, values_t)


def shards(
    query_proj,
    key_proj,
    value_proj,
    q_gain,
    k_gain,
    residual,
    out_weight,
    norm_gain,
    value_weight,
    gate_weight,
    down_weight,
    conv_value,
    conv_gate,
):
    tokens = query_proj.shape[0]
    heads_here = query_proj.shape[1] // HEAD_DIM
    kv_here = key_proj.shape[1] // HEAD_DIM
    group_size = heads_here // kv_here
    sp_size, tp_size = lax.axis_size("sp"), lax.axis_size("tp")
    count = math.gcd(sp_size, 4)
    stride = sp_size // count
    me, core = lax.axis_index("sp"), lax.axis_index("tp")
    place, rest = me // stride, me % stride
    positions = me * tokens + jnp.arange(tokens, dtype=jnp.int32)

    queries = grid_rotary(
        rms_norm(query_proj.reshape(tokens, heads_here, HEAD_DIM), q_gain), positions
    ) * HEAD_DIM ** (-0.5)
    queries = queries.astype(jnp.bfloat16)
    keys_rot = grid_rotary(
        rms_norm(key_proj.reshape(tokens, kv_here, HEAD_DIM), k_gain), positions
    ).astype(jnp.bfloat16)
    values = value_proj.reshape(tokens, kv_here, HEAD_DIM)

    ff_here = value_weight.shape[1]
    depth_here = value_weight.shape[0]
    hidden_here = ff_here // count

    split_heads = count if kv_here % count == 0 else 1
    kv_each = kv_here // split_heads
    packed = jnp.concatenate(
        [queries.reshape(tokens, kv_here, group_size * HEAD_DIM), keys_rot, values], axis=2
    ).transpose(1, 0, 2)
    packed = packed.reshape(split_heads, kv_each, tokens, (group_size + 2) * HEAD_DIM)
    if split_heads > 1:
        got = exchange_pieces(
            lambda at: lax.dynamic_index_in_dim(packed, at, 0, keepdims=False),
            place,
            count,
            stride,
            sp_size,
        )
        got, weights_in = lax.optimization_barrier((got, (value_weight, gate_weight, down_weight)))
    else:
        got, weights_in = [packed[0]], (value_weight, gate_weight, down_weight)
    value_in, gate_in, down_in = weights_in

    q_width = group_size * HEAD_DIM
    kv_mine = jnp.stack([piece[..., q_width:] for piece in got])
    if split_heads > 1:
        kv_all = jnp.stack(spread(kv_mine, count, stride))
    else:
        kv_all = lax.all_gather(kv_mine, "sp", axis=0)
    kv_all = kv_all.transpose(2 + 0, 0, 1, 3, 4).reshape(kv_each, sp_size * tokens, 2 * HEAD_DIM)

    def up_block(at):
        start = at * hidden_here
        return jnp.concatenate(
            [
                lax.dynamic_slice_in_dim(value_in, start, hidden_here, 1),
                lax.dynamic_slice_in_dim(gate_in, start, hidden_here, 1),
            ],
            axis=1,
        )

    def down_block(at):
        return lax.dynamic_slice_in_dim(down_in, at * hidden_here, hidden_here, 0)

    up_got = exchange_pieces(up_block, place, count, stride, sp_size)
    up_pieces = spread(in_place_order(up_got, place), count, stride)
    columns_here = down_weight.shape[1]
    down_got = exchange_pieces(down_block, place, count, stride, sp_size)
    down_cols = in_place_order(down_got, place).reshape(count, hidden_here, columns_here)
    down_cols = jnp.concatenate([down_cols[at] for at in range(count)], axis=1)
    down_pieces = spread(down_cols, count, stride)

    q_pieces = [piece[..., :q_width] for piece in got]
    per_head = []
    for kv_at in range(kv_each):
        keys_h = kv_all[kv_at, :, :HEAD_DIM]
        values_t = kv_all[kv_at, :, HEAD_DIM:].T
        per_group = []
        for group_at in range(group_size):
            columns = slice(group_at * HEAD_DIM, (group_at + 1) * HEAD_DIM)
            q_here = jnp.concatenate([piece[kv_at, :, columns] for piece in q_pieces], axis=0)
            per_group.append(attend(q_here, keys_h, values_t))
        per_head.append(jnp.concatenate(per_group, axis=1))
    done = jnp.concatenate(per_head, axis=1).reshape(len(got), tokens, -1)
    if split_heads > 1:
        back = [done[0]]
        for hop in range(1, count):
            back.append(lax.ppermute(done[hop], "sp", shifted(-hop, count, stride, sp_size)))
        attended = jnp.roll(jnp.stack(back), place, axis=0).transpose(1, 0, 2)
        attended = attended.reshape(tokens, heads_here * HEAD_DIM)
    else:
        attended = done[0]

    row_share = tokens // tp_size
    residual_mine = lax.dynamic_slice_in_dim(residual, core * row_share, row_share, 0)
    if tp_size == 2:
        weight_other = swap_cores(out_weight)
        halves = attended.reshape(2, row_share, heads_here * HEAD_DIM)
        rows_mine = lax.dynamic_index_in_dim(halves, core, 0, keepdims=False)
        rows_other = swap_cores(lax.dynamic_index_in_dim(halves, 1 - core, 0, keepdims=False))
        mix_mine = jnp.dot(rows_mine, out_weight, preferred_element_type=jnp.float32)
        mix_other = jnp.dot(rows_other, weight_other, preferred_element_type=jnp.float32)
        mix_out = (
            mix_mine.astype(jnp.bfloat16).astype(jnp.float32)
            + mix_other.astype(jnp.bfloat16).astype(jnp.float32)
        ).astype(jnp.bfloat16)
    else:
        mix_out = lax.psum_scatter(
            jnp.dot(attended, out_weight, preferred_element_type=jnp.float32).astype(jnp.bfloat16),
            "tp",
            scatter_dimension=0,
            tiled=True,
        )
    updated = (residual_mine.astype(jnp.float32) + mix_out.astype(jnp.float32)).astype(jnp.bfloat16)
    normed = rms_norm(updated, norm_gain).astype(jnp.bfloat16)
    width = normed.shape[1]
    normed = jnp.stack(
        [
            jnp.concatenate(
                [
                    normed[:, (at * stride + flip) * depth_here :][:, :depth_here]
                    for at in range(count)
                ],
                axis=1,
            )
            for flip in range(stride)
        ]
    )

    ups = []
    for hop in range(count):
        rows = normed
        if hop:
            rows = lax.ppermute(normed, "sp", shifted(hop, count, stride, sp_size))
        if tp_size == 2:
            other = swap_cores(rows)
            rows = jnp.concatenate(
                [jnp.where(core == 0, rows, other), jnp.where(core == 0, other, rows)], axis=1
            )
        else:
            rows = lax.all_gather(rows, "tp", axis=1, tiled=True)
        total = 0.0
        for flip in range(stride):
            part = lax.dynamic_index_in_dim(rows, rest ^ flip, 0, keepdims=False)
            total = total + jnp.dot(part, up_pieces[flip], preferred_element_type=jnp.float32)
        ups.append(total.astype(jnp.bfloat16))
    ups = jnp.stack(ups)

    forward = [
        (group * stride + at, group * stride + (at + 1) % stride)
        for group in range(count)
        for at in range(stride)
    ]
    backward = [(target, source) for source, target in forward]
    before = lax.ppermute(ups[:, -1], "sp", forward)
    after = lax.ppermute(ups[:, 0], "sp", backward)
    hops = jnp.arange(count)
    block_at = (place - hops) % count
    no_before = (rest == 0) & (block_at == 0)
    no_after = (rest == stride - 1) & (block_at == count - 1)
    before = jnp.where(rest == 0, jnp.roll(before, -1, axis=0), before)
    after = jnp.where(rest == stride - 1, jnp.roll(after, 1, axis=0), after)
    before = jnp.where(no_before[:, None], 0, before)
    after = jnp.where(no_after[:, None], 0, after)
    padded = jnp.concatenate([before[:, None], ups, after[:, None]], axis=1).astype(jnp.float32)
    taps = jnp.concatenate(
        [
            lax.dynamic_slice_in_dim(conv_value, place * hidden_here, hidden_here, 1),
            lax.dynamic_slice_in_dim(conv_gate, place * hidden_here, hidden_here, 1),
        ],
        axis=1,
    )
    conv = padded[:, :-2] * taps[0] + padded[:, 1:-1] * taps[1] + padded[:, 2:] * taps[2]
    hidden = (
        jax.nn.gelu(conv[..., hidden_here:], approximate=True) * conv[..., :hidden_here]
    ).astype(jnp.bfloat16)

    down_all = jnp.concatenate(down_pieces, axis=1)
    branch = 0.0
    for hop in list(range(1, count)) + [0]:
        partial = jnp.dot(hidden[hop], down_all, preferred_element_type=jnp.float32)
        if tp_size == 2:
            partial = partial.reshape(2, row_share, width)
            mine = lax.dynamic_index_in_dim(partial, core, 0, keepdims=False)
            theirs = lax.dynamic_index_in_dim(partial, 1 - core, 0, keepdims=False)
            other = swap_cores(theirs.astype(jnp.bfloat16))
            mine = mine + other.astype(jnp.float32)
        else:
            mine = lax.psum_scatter(
                partial.astype(jnp.bfloat16), "tp", scatter_dimension=0, tiled=True
            )
        if hop:
            mine = lax.ppermute(
                mine.astype(jnp.bfloat16), "sp", shifted(-hop, count, stride, sp_size)
            )
        branch = branch + mine.astype(jnp.float32)
    branch = branch.astype(jnp.bfloat16)
    span = count * columns_here
    pieces = unflip([branch[:, at * span : (at + 1) * span] for at in range(stride)], rest)
    branch = jnp.concatenate(
        [
            pieces[at][:, group * columns_here : (group + 1) * columns_here]
            for group in range(count)
            for at in range(stride)
        ],
        axis=1,
    )
    return (updated.astype(jnp.float32) + branch.astype(jnp.float32)).astype(jnp.bfloat16)


def fused_kernel(
    query, key, value, q_gain, k_gain, cosine, sine, res_in, wo_in, gain, wv_in, wg_in, wd_in, taps_v, taps_g, out, upd_out,
    q_in, kv_in, qraw, qhead, kvbuf, kbuf, vbuf, top, total, acc, att_send, att_all, wo, res, mix_send, mix_recv,
    own_mix, upd, rows, wup, wdown, ups, hidden, part_keep, part_send, part_recv, red_send,
    red_recv, fin, local_sem, send_sem, recv_sem,
):
    sp, core = lax.axis_index("sp"), lax.axis_index("tp")
    x, y, zl, zh = sp % 2, (sp // 2) % 2, (sp // 4) % 2, sp // 8
    fx, fy, fl, fh = 1 - 2 * x, 1 - 2 * y, 1 - 2 * zl, 1 - 2 * zh
    depth = wv_in.shape[0]
    ffs = wdown.shape[1]
    pairs, half, pair_w = upd.shape
    tokens = 2 * half
    other = 1 - core

    def xs(flip):
        return x + fx * flip

    def mate(at):
        return sp + fx * (at % 2) + 4 * fl * (at // 2)

    def place(at):
        return xs(at % 2) + 2 * (zl + fl * (at // 2))

    mine = place(0)
    y_mate, z_mate = sp + 2 * fy, sp + 8 * fh
    diag_mate = sp + 2 * fy + 8 * fh

    def pair_at(rel):
        return (y + fy * (rel % 2)) + 2 * (zl + fl * ((rel // 2) % 2)) + 4 * (zh + fh * (rel // 4))

    ids = {}
    started = []

    def remote(name, src, dst, device):
        at = ids.setdefault(name, len(ids))
        assert at < send_sem.shape[0], len(ids)
        return pltpu.make_async_remote_copy(
            src_ref=src, dst_ref=dst, send_sem=send_sem.at[at], recv_sem=recv_sem.at[at],
            device_id=device, device_id_type=pl.DeviceIdType.MESH,
        )

    def send(name, src, dst, device):
        copy = remote(name, src, dst, device)
        copy.start()
        started.append(copy)

    def arrived(name, dst):
        remote(name, dst, dst, (sp, core)).wait_recv()

    def lanes(start, size):
        return pl.ds(pl.multiple_of(start, 128), size)

    barrier = pltpu.get_barrier_semaphore()
    partners = [(sp, other)] + [(mate(at), core) for at in (1, 2, 3)]
    partners += [(y_mate, core), (z_mate, core), (diag_mate, core)]
    for device in partners:
        pl.semaphore_signal(barrier, inc=1, device_id=device, device_id_type=pl.DeviceIdType.MESH)

    lane = lax.broadcasted_iota(jnp.int32, (tokens, 2 * HEAD_DIM), 1)
    left_head = lane < HEAD_DIM
    quarter = HEAD_DIM // 4
    low = lane % (2 * quarter) < quarter
    lanes_all = 2 * HEAD_DIM
    q_row, k_row = (jnp.concatenate([ref[...], ref[...]], axis=1) for ref in (q_gain, k_gain))

    def spread_table(table):
        grid_rows = table.shape[0] - GRID_W
        columns = table[grid_rows:, :]
        in_first = lane[:GRID_W] % HEAD_DIM < HEAD_DIM // 2
        parts = [jnp.where(in_first, table[r : r + 1, :], columns) for r in range(grid_rows)]
        return jnp.concatenate(parts, axis=0)

    turn_c, turn_s = spread_table(cosine), spread_table(sine)

    def rotate(heads_pair, gain_row, scale):
        wide = heads_pair.astype(jnp.float32)
        squares = wide * wide
        left = jnp.sum(jnp.where(left_head, squares, 0.0), axis=1, keepdims=True)
        right = jnp.sum(jnp.where(left_head, 0.0, squares), axis=1, keepdims=True)
        mean = jnp.where(left_head, left, right) / HEAD_DIM
        normed = wide * lax.rsqrt(mean + NORM_EPS) * gain_row
        swapped = jnp.where(
            low,
            pltpu.roll(normed, lanes_all - quarter, 1),
            pltpu.roll(normed, quarter, 1),
        )
        return (normed * turn_c + swapped * turn_s) * scale

    for m in range(key.shape[1] // lanes_all):
        cols = slice(m * lanes_all, (m + 1) * lanes_all)
        turned = rotate(key[:, cols], k_row, 1.0)
        passed = value[:, cols].astype(jnp.float32)
        first = jnp.where(left_head, turned, pltpu.roll(passed, HEAD_DIM, 1))
        second = jnp.where(left_head, pltpu.roll(turned, HEAD_DIM, 1), passed)
        kv_in[2 * m] = first.astype(jnp.bfloat16)
        kv_in[2 * m + 1] = second.astype(jnp.bfloat16)
    pl.semaphore_wait(barrier, len(partners))

    def piece(kind, rel, x_at):
        start = pl.multiple_of(x_at * depth, depth)
        if kind == "v":
            return wup.at[rel, pl.ds(start, depth), pl.ds(0, ffs)]
        if kind == "g":
            return wup.at[rel, pl.ds(start, depth), pl.ds(ffs, ffs)]
        return wdown.at[rel, :, pl.ds(start, depth)]

    def whole(kind, rel):
        if kind == "v":
            return wup.at[rel, :, pl.ds(0, ffs)]
        if kind == "g":
            return wup.at[rel, :, pl.ds(ffs, ffs)]
        return wdown.at[rel]

    def shard(kind, at):
        if kind == "d":
            return wd_in.at[pl.ds(pl.multiple_of(place(at) * ffs, 128), ffs), :]
        return (wv_in if kind == "v" else wg_in).at[:, lanes(place(at) * ffs, ffs)]

    def launch(name, src, dst, device, where):
        fresh = name not in ids
        copy = remote(name, src, dst, device)
        if where is None:
            copy.start()
        else:
            pl.when(where)(copy.start)
        if fresh:
            started.append(copy)

    def exchange(kind, at, where=None):
        dst = piece(kind, 2 * (at // 2), x)
        launch(f"w1{kind}{at}", shard(kind, at), dst, (mate(at), core), where)

    def exchanged(kind, at):
        arrived(f"w1{kind}{at}", piece(kind, 2 * (at // 2), xs(at % 2)))

    inner, outer = zl != zh, zl == zh

    def across(kind, at, where=None):
        src = piece(kind, 2 * (at // 2), xs(at % 2)) if at else shard(kind, 0)
        dst = piece(kind, 2 * (at // 2) + 4, xs(at % 2))
        launch(f"wz{kind}{at}", src, dst, (z_mate, core), where)

    def crossed(kind, at):
        arrived(f"wz{kind}{at}", piece(kind, 2 * (at // 2) + 4, xs(at % 2)))

    def sideways(kind, rel, where=None):
        launch(f"wy{kind}{rel}", whole(kind, rel), whole(kind, rel + 1), (y_mate, core), where)

    def sideways_half(kind, at):
        src = piece(kind, 0, xs(at)) if at else shard(kind, 0)
        send(f"wy{kind}h{at}", src, piece(kind, 1, xs(at)), (y_mate, core))

    def from_side(kind, rel):
        if rel or kind == "d":
            arrived(f"wy{kind}{rel}", whole(kind, rel + 1))
        else:
            arrived(f"wy{kind}h0", piece(kind, 1, x))
            arrived(f"wy{kind}h1", piece(kind, 1, xs(1)))

    for at in (2, 3, 1):
        send(f"kv{at}", kv_in.at[place(at)], kvbuf.at[0, mine], (mate(at), core))
    for m in range(q_in.shape[0]):
        cols = slice(m * lanes_all, (m + 1) * lanes_all)
        q_in[m] = rotate(query[:, cols], q_row, HEAD_DIM ** (-0.5)).astype(jnp.bfloat16)
    for at in (2, 3, 1):
        send(f"q{at}", q_in.at[place(at)], qraw.at[mine], (mate(at), core))
    locals_ = [
        pltpu.make_async_copy(shard(kind, 0), piece(kind, 0, x), local_sem.at[n])
        for n, kind in enumerate("vgd")
    ]
    locals_.append(pltpu.make_async_copy(wo_in, wo, local_sem.at[3]))
    locals_.append(
        pltpu.make_async_copy(
            res_in.at[pl.ds(pl.multiple_of(core * half, half), half), :], res, local_sem.at[4]
        )
    )
    for copy in locals_:
        copy.start()
    qraw[mine] = q_in[mine]
    kvbuf[0, mine] = kv_in[mine]
    top[...] = jnp.full(top.shape, -1e30, jnp.float32)
    total[...] = jnp.zeros(total.shape, jnp.float32)
    acc[...] = jnp.zeros(acc.shape, jnp.float32)
    for at in (1, 2, 3):
        arrived(f"kv{at}", kvbuf.at[0, place(at)])
    send("kvz", kvbuf.at[0], kvbuf.at[2], (z_mate, core))
    send("kvy", kvbuf.at[0], kvbuf.at[1], (y_mate, core))
    sideways_half("v", 0)
    for at in (1, 2, 3):
        arrived(f"q{at}", qraw.at[place(at)])
    across("v", 0)
    for at in (1, 2, 3):
        exchange("v", at)
    sideways_half("g", 0)
    for at in (2, 3, 1):
        exchange("g", at)
    width = HEAD_DIM
    group = qraw.shape[2] // width
    blocks = qraw.shape[0]

    @pl.loop(0, blocks)
    def _(b):
        for a in range(group):
            qhead[b * group + a] = qraw[b][:, a * width : (a + 1) * width]

    def unpack(t):
        @pl.loop(0, blocks)
        def _(b):
            start = pl.multiple_of(b * tokens, tokens)
            pair = kvbuf[t, b]
            kbuf[t, pl.ds(start, tokens), :] = pair[:, :width]
            vbuf[t, :, pl.ds(start, tokens)] = pair[:, width:].T

    def attend_block(t, h):
        scores = lax.dot_general(
            kbuf[t], qhead[h], (((1,), (1,)), ((), ())), preferred_element_type=jnp.float32
        )
        old = top[h]
        new = jnp.maximum(old, jnp.max(scores, axis=0, keepdims=True))
        probs = jnp.exp(scores - new)
        shrink = jnp.exp(old - new)
        total[h] = total[h] * shrink + jnp.sum(probs, axis=0, keepdims=True)
        acc[h] = acc[h] * shrink + jnp.dot(
            vbuf[t], probs.astype(jnp.bfloat16), preferred_element_type=jnp.float32
        )
        top[h] = new

    def attend_some(t, lo, hi):
        @pl.loop(lo, hi)
        def _(h):
            attend_block(t, h)

    heads = blocks * group
    unpack(0)
    attend_some(0, 0, heads // 2)
    for copy in locals_[:3]:
        copy.wait()
    exchanged("v", 1)
    across("v", 1)
    sideways_half("v", 1)
    across("g", 0)
    attend_some(0, heads // 2, heads)
    arrived("kvy", kvbuf.at[1])
    unpack(1)
    attend_some(1, 0, heads // 2)
    exchanged("g", 1)
    across("g", 1)
    sideways_half("g", 1)
    attend_some(1, heads // 2, heads)
    arrived("kvz", kvbuf.at[2])
    send("kvd", kvbuf.at[2], kvbuf.at[3], (y_mate, core))
    unpack(2)
    attend_some(2, 0, heads // 2)
    exchanged("v", 2)
    exchanged("v", 3)
    sideways("v", 2)
    across("v", 2)
    across("v", 3)
    attend_some(2, heads // 2, heads)
    arrived("kvd", kvbuf.at[3])
    unpack(3)

    def finish(block):
        first = block * group
        pieces = [acc[first + a] / total[first + a] for a in range(group)]
        return jnp.concatenate(pieces, axis=0).T.astype(jnp.bfloat16)

    for at in (2, 3, 1, 0):
        block = place(at)
        attend_some(3, block * group, block * group + group)
        if at:
            att_send[at - 1] = finish(block)
            send(f"att{at}", att_send.at[at - 1], att_all.at[mine], (mate(at), core))
        else:
            att_all[mine] = finish(block)
    exchanged("g", 2)
    exchanged("g", 3)
    sideways("g", 2)
    exchange("d", 1)
    for copy in locals_[3:]:
        copy.wait()
    for at in (1, 2, 3):
        arrived(f"att{at}", att_all.at[place(at)])
    crossed("v", 0)
    crossed("v", 1)
    sideways("v", 4)

    def project(n, rows_at):
        start = pl.multiple_of(rows_at * half, half)
        left = jnp.concatenate([att_all[b, pl.ds(start, half), :] for b in range(blocks)], axis=1)
        return jnp.dot(left, wo[:, lanes(n * pair_w, pair_w)], preferred_element_type=jnp.float32)

    @pl.loop(0, pairs)
    def _(n):
        mix_send[n] = project(n, other).astype(jnp.bfloat16)

    send("mix", mix_send, mix_recv, (sp, other))

    @pl.loop(0, pairs)
    def _(n):
        own_mix[n] = project(n, core).astype(jnp.bfloat16)

    arrived("mix", mix_recv)

    def update(n, squares):
        mixed = own_mix[n].astype(jnp.float32) + mix_recv[n].astype(jnp.float32)
        mixed = mixed.astype(jnp.bfloat16).astype(jnp.float32)
        held = res[:, lanes(n * pair_w, pair_w)].astype(jnp.float32)
        new = (held + mixed).astype(jnp.bfloat16)
        upd[n] = new
        upd_out[:, lanes(n * pair_w, pair_w)] = new
        wide = new.astype(jnp.float32)
        return squares + jnp.sum(wide * wide, axis=1, keepdims=True)

    squares = lax.fori_loop(0, pairs, update, jnp.zeros((half, 1), jnp.float32))
    inv = lax.rsqrt(squares / (pairs * pair_w) + NORM_EPS)
    my_rows = pl.ds(pl.multiple_of(core * half, half), half)

    @pl.loop(0, pairs)
    def _(n):
        scaled = upd[n].astype(jnp.float32) * inv * gain[:, lanes(n * pair_w, pair_w)]
        rows[mine, n, my_rows, :] = scaled.astype(jnp.bfloat16)

    def rows_of(g, at, part=None):
        cut = slice(None) if part is None else pl.ds(part * (pairs // 2), pairs // 2)
        return rows.at[g, cut, pl.ds(pl.multiple_of(at * half, half), half), :]

    def spread_rows(name, at_block, device, part=None):
        ref = rows_of(place(at_block), core, part)
        send(name, ref, ref, device)

    for part in (0, 1):
        spread_rows(f"row2{part}", 0, (mate(2), core), part)
        spread_rows(f"row1{1 - part}", 0, (mate(1), core), 1 - part)
    spread_rows("row0", 0, (sp, other))
    across("g", 2, outer)
    across("g", 3, outer)

    def up_dot(g, rels):
        left = jnp.concatenate([rows[g, pair_at(rel)] for rel in rels], axis=1)
        return left

    def up_block(g, rels, fresh):
        up_inner(g, rels, fresh)

    def up_inner(g, rels, fresh):
        seg, x_at = g // 2, g % 2
        start = pl.multiple_of(8 + x_at * tokens, 8)
        left = up_dot(g, rels)

        @pl.loop(0, 2 * ffs // pair_w)
        def _(n):
            cols = lanes(n * pair_w, pair_w)
            part = jnp.zeros((tokens, pair_w), jnp.float32)
            for i, rel in enumerate(rels):
                part = part + jnp.dot(
                    left[:, i * pair_w : (i + 1) * pair_w], wup[rel, :, cols],
                    preferred_element_type=jnp.float32,
                )
            if fresh:
                ups[seg, pl.ds(start, tokens), cols] = part
            else:
                ups[seg, pl.ds(start, tokens), cols] += part

    for kind in "vg":
        from_side(kind, 0)
        from_side(kind, 2)
    arrived("row0", rows_of(mine, other))
    up_block(mine, (0, 2, 1, 3), True)
    crossed("g", 0)
    crossed("g", 1)
    sideways("g", 4)
    arrived("row20", rows_of(place(2), core, 0))
    spread_rows("row30", 2, (mate(1), core), 0)
    arrived("row11", rows_of(place(1), core, 1))
    spread_rows("row31", 1, (mate(2), core), 1)
    exchanged("d", 1)
    across("d", 0, outer)
    across("d", 1, outer)
    for at in (2, 3):
        exchange("d", at, outer)
    arrived("row21", rows_of(place(2), core, 1))
    spread_rows("fwd2", 2, (sp, other))
    arrived("row10", rows_of(place(1), core, 0))
    spread_rows("fwd1", 1, (sp, other))
    sideways("d", 0)
    arrived("fwd2", rows_of(place(2), other))
    up_block(place(2), (0, 2, 1, 3), True)
    crossed("v", 2)
    crossed("v", 3)
    sideways("v", 6)
    across("g", 2, inner)
    across("g", 3, inner)
    for at in (2, 3):
        exchange("d", at, inner)
    arrived("fwd1", rows_of(place(1), other))
    up_block(place(1), (0, 2, 1, 3), True)
    arrived("row30", rows_of(place(3), core, 0))
    arrived("row31", rows_of(place(3), core, 1))
    spread_rows("fwd3", 3, (sp, other))
    across("d", 0, inner)
    across("d", 1, inner)
    arrived("fwd3", rows_of(place(3), other))
    up_block(place(3), (0, 2, 1, 3), True)
    crossed("g", 2)
    crossed("g", 3)
    sideways("g", 6)

    @pl.loop(0, blocks)
    def _(g):
        up_block(g, (4, 6), False)

    @pl.when(inner)
    def _():
        exchanged("d", 2)
        exchanged("d", 3)

    across("d", 2, inner)
    across("d", 3, inner)
    sideways("d", 2, inner)
    for kind in "vg":
        from_side(kind, 4)
        from_side(kind, 6)


    @pl.loop(0, blocks)
    def _(g):
        up_block(g, (5, 7), False)

    span = 2 * tokens
    head, tail = pl.ds(8, 8), pl.ds(span, 8)
    before, after = pl.ds(0, 8), pl.ds(span + 8, 8)
    even = y == 0

    def edge(name, seg_from, rows_from, seg_to, rows_to, device):
        send_at = remote(name, ups.at[seg_from, rows_from, :], ups.at[seg_to, rows_to, :], device)
        return send_at

    @pl.when(even)
    def _():
        edge("h0", 1, head, 0, after, (y_mate, core)).start()
        edge("h1", 0, tail, 0, before, (y_mate, core)).start()
        edge("h2", 1, tail, 1, before, (y_mate, core)).start()

        @pl.when(zh == 1)
        def _():
            edge("h3", 0, head, 1, after, (diag_mate, core)).start()

        @pl.when(zh == 0)
        def _():
            ups[0, before, :] = jnp.zeros((8, 2 * ffs), jnp.float32)

    @pl.when(y == 1)
    def _():
        edge("h0", 0, head, 0, after, (y_mate, core)).start()
        edge("h1", 1, head, 1, after, (y_mate, core)).start()
        edge("h2", 0, tail, 1, before, (y_mate, core)).start()

        @pl.when(zh == 0)
        def _():
            edge("h3", 1, tail, 0, before, (diag_mate, core)).start()

        @pl.when(zh == 1)
        def _():
            ups[1, after, :] = jnp.zeros((8, 2 * ffs), jnp.float32)

    tap_cols = lanes(mine * ffs, ffs)
    tv, tg = taps_v[:, tap_cols], taps_g[:, tap_cols]
    step = 64

    def convolve(window, taps):
        rounded = window.astype(jnp.bfloat16).astype(jnp.float32)
        return (
            rounded[7 : 7 + step] * taps[0:1]
            + rounded[8 : 8 + step] * taps[1:2]
            + rounded[9 : 9 + step] * taps[2:3]
        )

    def hidden_block(i):
        seg, at = i // (span // step), i % (span // step)
        window = pl.ds(pl.multiple_of(at * step, 8), step + 16)
        for n in range(ffs // 128):
            left, right = slice(n * 128, n * 128 + 128), slice(ffs + n * 128, ffs + n * 128 + 128)
            conv_v = convolve(ups[seg, window, left], tv[:, left])
            conv_g = convolve(ups[seg, window, right], tg[:, left])
            value = jax.nn.gelu(conv_g, approximate=True) * conv_v
            block, at_row = i // (tokens // step), (i % (tokens // step)) * step
            to = (at_row // half) * blocks * half + block * half + at_row % half
            hidden[pl.ds(pl.multiple_of(to, step), step), left] = value.astype(jnp.bfloat16)

    per = span // step

    @pl.loop(0, 2 * (per - 2))
    def _(i):
        seg = i // (per - 2)
        hidden_block(seg * per + 1 + i % (per - 2))

    @pl.when(even)
    def _():
        edge("h0", 0, head, 0, after, (sp, core)).wait_recv()
        edge("h1", 1, head, 1, after, (sp, core)).wait_recv()
        edge("h2", 0, tail, 1, before, (sp, core)).wait_recv()

        @pl.when(zh == 1)
        def _():
            edge("h3", 1, tail, 0, before, (sp, core)).wait_recv()

    @pl.when(y == 1)
    def _():
        edge("h0", 1, head, 0, after, (sp, core)).wait_recv()
        edge("h1", 0, tail, 0, before, (sp, core)).wait_recv()
        edge("h2", 1, tail, 1, before, (sp, core)).wait_recv()

        @pl.when(zh == 0)
        def _():
            edge("h3", 0, head, 1, after, (sp, core)).wait_recv()

    @pl.when(outer)
    def _():
        exchanged("d", 2)
        exchanged("d", 3)

    across("d", 2, outer)
    across("d", 3, outer)
    sideways("d", 2, outer)
    crossed("d", 0)
    crossed("d", 1)
    sideways("d", 4)

    @pl.loop(0, 4)
    def _(i):
        hidden_block((i // 2) * per + (i % 2) * (per - 1))

    order = [0, 2, 1, 3, 4, 6, 5, 7]
    straight = order[-4:]

    def down(rel):
        def product(at):
            left = hidden[pl.ds(pl.multiple_of(at * blocks * half, half), blocks * half), :]
            whole_part = jnp.dot(left, wdown[rel], preferred_element_type=jnp.float32)
            return whole_part.reshape(blocks, half, pair_w)

        part_send[rel] = product(other).astype(jnp.bfloat16)
        send(f"part{rel}", part_send.at[rel], part_recv.at[rel], (sp, other))
        part_keep[order.index(rel) % 2] = product(core)

    def merge(rel):
        arrived(f"part{rel}", part_recv.at[rel])

        def both(at):
            g = place(at)
            return part_keep[order.index(rel) % 2, g] + part_recv[rel, g].astype(jnp.float32)

        if rel in straight:
            for at in (2, 3, 1):
                red_send[rel, at - 1] = both(at).astype(jnp.bfloat16)
                to = across_rel(rel, at)
                send(f"red{to}{at}", red_send.at[rel, at - 1], red_recv.at[to, at - 1],
                     (mate(at), core))
            fin[rel, 0] = both(0)
            return
        first, second = ways()
        for i, at in enumerate((first, 3)):
            red_send[rel, i] = both(at).astype(jnp.bfloat16)
        to = across_rel(rel, first)
        send(f"reda{to}", red_send.at[rel, pl.ds(0, 2)], red_recv.at[to, pl.ds(0, 2)],
             (mate(first), core))
        fin[rel, 0] = both(0)
        fin[rel, 1] = both(second)

    def ways():
        return (1, 2)

    def across_rel(rel, at):
        return rel ^ (at & 2)

    def pass_on(rel):
        second = ways()[1]
        arrived(f"reda{rel}", red_recv.at[rel, pl.ds(0, 2)])
        red_send[rel, 2] = (fin[rel, 1] + red_recv[rel, 1].astype(jnp.float32)).astype(jnp.bfloat16)
        to = across_rel(rel, second)
        send(f"redb{to}", red_send.at[rel, 2], red_recv.at[to, 2], (mate(second), core))

    def close(rel):
        branch = fin[rel, 0]
        if rel in straight:
            for at in (1, 2, 3):
                arrived(f"red{rel}{at}", red_recv.at[rel, at - 1])
                branch = branch + red_recv[rel, at - 1].astype(jnp.float32)
        else:
            arrived(f"redb{rel}", red_recv.at[rel, 2])
            branch = branch + red_recv[rel, 0].astype(jnp.float32)
            branch = branch + red_recv[rel, 2].astype(jnp.float32)
        n = pair_at(rel)
        out[:, lanes(n * pair_w, pair_w)] = branch.astype(jnp.bfloat16)

    down(0)
    for i, rel in enumerate(order[1:]):
        if rel == 1:
            from_side("d", 0)
        if rel == 3:
            from_side("d", 2)
        if rel == 4:
            crossed("d", 2)
            crossed("d", 3)
            sideways("d", 6)
        if rel == 5:
            from_side("d", 4)
        if rel == 7:
            from_side("d", 6)
        down(rel)
        merge(order[i])
        if i >= 2 and order[i - 2] not in straight:
            pass_on(order[i - 2])
    merge(order[-1])
    for rel in order:
        close(rel)
    for copy in started:
        copy.wait_send()
    for name in ("h0", "h1", "h2"):
        edge(name, 0, head, 0, after, (sp, core)).wait_send()

    @pl.when((y + zh) == 1)
    def _():
        edge("h3", 0, head, 0, after, (sp, core)).wait_send()


def fused(query_proj, key_proj, value_proj, gains, tables, residual, out_weight, norm_gain,
          value_weight, gate_weight, down_weight, conv_value, conv_gate):
    groups, tokens = key_proj.shape[1] // HEAD_DIM, query_proj.shape[0]
    q_width = query_proj.shape[1] // groups
    half, width = tokens // 2, residual.shape[1]
    depth, ff_here = value_weight.shape
    pair_w = 2 * depth
    pairs = width // pair_w
    ffs = ff_here // groups
    heads = groups * (q_width // HEAD_DIM)
    keys = groups * tokens
    bf16, f32 = jnp.bfloat16, jnp.float32
    vmem, anywhere = pl.BlockSpec(memory_space=pltpu.VMEM), pl.BlockSpec(memory_space=pl.ANY)
    copies = 104
    return pl.pallas_call(
        fused_kernel,
        out_shape=[jax.ShapeDtypeStruct((half, width), bf16)] * 2,
        in_specs=[vmem] * 7 + [anywhere, anywhere, vmem, anywhere, anywhere, anywhere, vmem, vmem],
        out_specs=[vmem, vmem],
        scratch_shapes=[
            pltpu.VMEM((groups, tokens, q_width), bf16),
            pltpu.VMEM((groups, tokens, 2 * HEAD_DIM), bf16),
            pltpu.VMEM((groups, tokens, q_width), bf16),
            pltpu.VMEM((heads, tokens, HEAD_DIM), bf16),
            pltpu.VMEM((4, groups, tokens, 2 * HEAD_DIM), bf16),
            pltpu.VMEM((4, keys, HEAD_DIM), bf16),
            pltpu.VMEM((4, HEAD_DIM, keys), bf16),
            pltpu.VMEM((heads, 1, tokens), f32),
            pltpu.VMEM((heads, 1, tokens), f32),
            pltpu.VMEM((heads, HEAD_DIM, tokens), f32),
            pltpu.VMEM((groups - 1, tokens, q_width), bf16),
            pltpu.VMEM((groups, tokens, q_width), bf16),
            pltpu.VMEM(out_weight.shape, bf16),
            pltpu.VMEM((half, width), bf16),
            pltpu.VMEM((pairs, half, pair_w), bf16),
            pltpu.VMEM((pairs, half, pair_w), bf16),
            pltpu.VMEM((pairs, half, pair_w), bf16),
            pltpu.VMEM((pairs, half, pair_w), bf16),
            pltpu.VMEM((groups, pairs, tokens, pair_w), bf16),
            pltpu.VMEM((pairs, pair_w, 2 * ffs), bf16),
            pltpu.VMEM((pairs, ffs, pair_w), bf16),
            pltpu.VMEM((2, 2 * tokens + 16, 2 * ffs), f32),
            pltpu.VMEM((keys, ffs), bf16),
            pltpu.VMEM((2, groups, half, pair_w), f32),
            pltpu.VMEM((pairs, groups, half, pair_w), bf16),
            pltpu.VMEM((pairs, groups, half, pair_w), bf16),
            pltpu.VMEM((pairs, groups - 1, half, pair_w), bf16),
            pltpu.VMEM((pairs, groups - 1, half, pair_w), bf16),
            pltpu.VMEM((pairs, 2, half, pair_w), f32),
            pltpu.SemaphoreType.DMA((5,)),
            pltpu.SemaphoreType.DMA((copies,)),
            pltpu.SemaphoreType.DMA((copies,)),
        ],
        compiler_params=pltpu.CompilerParams(
            collective_id=0, has_side_effects=True, vmem_limit_bytes=60 * 2**20
        ),
    )(query_proj, key_proj, value_proj, *gains, *tables, residual, out_weight, norm_gain[None, :], value_weight, gate_weight,
      down_weight, conv_value, conv_gate)


def fused_layer(
    query_proj, key_proj, value_proj, q_gain, k_gain, residual, out_weight, norm_gain,
    value_weight, gate_weight, down_weight, conv_value, conv_gate,
):
    tokens, width = query_proj.shape[0], 2 * HEAD_DIM
    grid_rows = tokens // GRID_W
    half = HEAD_DIM // 2
    frequency = ROPE_BASE ** (-np.arange(0, half, 2, dtype=np.float32) / half)
    frequency = np.tile(frequency.astype(np.float32), width // (half // 2))[None, :]
    at = lax.broadcasted_iota(jnp.int32, (grid_rows + GRID_W, width), 0)
    place = jnp.where(at < grid_rows, lax.axis_index("sp") * grid_rows + at, at - grid_rows)
    angle = place.astype(jnp.float32) * frequency
    lane = lax.broadcasted_iota(jnp.int32, at.shape, 1)
    sign = jnp.where(lane % half < half // 2, -1.0, 1.0)
    tables = (jnp.cos(angle), jnp.sin(angle) * sign)
    gains = (q_gain[None, :], k_gain[None, :])
    branch, updated = fused(
        query_proj, key_proj, value_proj, gains, tables, residual, out_weight, norm_gain,
        value_weight, gate_weight, down_weight, conv_value, conv_gate,
    )
    return (updated.astype(jnp.float32) + branch.astype(jnp.float32)).astype(jnp.bfloat16)


def fits(sp_size, tp_size, arrays):
    tokens, kv_here = arrays[0].shape[0], arrays[1].shape[1] // HEAD_DIM
    depth, ff_here = arrays[8].shape
    return (
        (sp_size, tp_size, kv_here) == (16, 2, 4)
        and depth % 128 == 0
        and arrays[0].shape[1] == 2 * arrays[1].shape[1]
        and ff_here % (kv_here * 128) == 0
        and (2 * ff_here // kv_here) % (2 * depth) == 0
        and tokens % 256 == 0
        and tokens % GRID_W == 0
    )


def layer(*arrays):
    if fits(lax.axis_size("sp"), lax.axis_size("tp"), arrays):
        return fused_layer(*arrays)
    return shards(*arrays)


def solution(mesh):
    return jax.shard_map(
        layer,
        mesh=mesh,
        in_specs=(
            P("sp", "tp"),
            P("sp", "tp"),
            P("sp", "tp"),
            P(),
            P(),
            P("sp", None),
            P("tp", None),
            P(),
            P("sp", "tp"),
            P("sp", "tp"),
            P("tp", "sp"),
            P(None, "tp"),
            P(None, "tp"),
        ),
        out_specs=P(("sp", "tp"), None),
        check_vma=False,
    )
```
